32 devices in a mesh: sp: 8 (over z, y), tp: 4 (over x, core).
Axes of the slice: x: 2, y: 2, z: 4, core: 2. Of those that a mesh axis runs over, the one named last changes fastest.
Arguments:
- queries: bfloat16 [6144, 1024], P('sp', 'tp'), may hold values from -6 to 6
- keys: bfloat16 [6144, 1024], P('sp', 'tp'), may hold values from -6 to 6
- values: bfloat16 [6144, 2048], P('sp', 'tp'), may hold values from -6 to 6
- out_gate: bfloat16 [6144, 2048], P('sp', 'tp'), may hold values from -6 to 6
- input_gates: float32 [2, 4, 6144], P(None, 'tp', 'sp'), may hold values from -4 to 300
- forget_gates: float32 [2, 4, 6144], P(None, 'tp', 'sp'), may hold values from -1 to 16
- doc_ids: int32 [6144], P('sp'), may hold values from 0 to 3, never falling along the last dimension, each value on 1 to 3072 neighbouring positions
- head_gain: float32 [2048], P('tp'), may hold values from 0.1 to 1.9
- w_out: bfloat16 [2048, 2048], P('tp'), may hold values from -0.25 to 0.25
- resid: bfloat16 [6144, 2048], P(('sp', 'tp')), may hold values from -30 to 30
- norm_gain: float32 [2048], replicated, may hold values from 0.1 to 1.9
- w_up: bfloat16 [2048, 8192], P('sp', 'tp'), may hold values from -0.125 to 0.125
- w_down: bfloat16 [8192, 2048], P('tp', 'sp'), may hold values from -0.0625 to 0.0625
Outputs:
- layer_out: bfloat16 [6144, 2048], P(('sp', 'tp'))
The draws below stay inside these ranges and needn't reach their ends.
Inputs may be any that keep to these rules, and one draw needn't show every extreme that they name: `doc_ids`: document numbers never fall along the positions.
All inputs are finite; a program needn't handle non-finite values.
Results may differ from the reference program's by a relative error of at most 0.013.
Values may be sent and summed in bfloat16 or wider, within the bound.
A program may use at most 128 MiB of HBM per device.

```python
import math
import jax
import jax.numpy as jnp
import numpy as np
from jax import lax

D = 2048
HEADS = 4
DQK = 256
DV = 512
FF = 8192
TOK_DEV = 768
TOKENS = 6144
N_SP = 8


def draw_resid(key, part):
    keys = jax.random.split(key, 2)
    base = jax.random.normal(keys[0], (TOKENS, D), jnp.float32)
    rows = jnp.exp(jax.random.uniform(keys[1], (TOKENS, 1), jnp.float32, -1.2, 1.2))
    cols = jnp.exp(jnp.linspace(-0.9, 0.9, D, dtype=jnp.float32))[None, :]
    return jnp.clip(base * rows * cols, -30.0, 30.0).astype(jnp.bfloat16)


def draw_input_gates(key, part):
    keys = jax.random.split(key, 1)
    gates = jnp.clip(jax.random.normal(keys[0], (2, HEADS, TOKENS), jnp.float32), -4.0, 4.0)
    return gates


def draw_forget_gates(key, part):
    keys = jax.random.split(key, 6)
    share = 0.5
    slow = jax.random.uniform(keys[0], (2, HEADS, 1), jnp.float32) < share
    fast_rate = jnp.exp(jax.random.uniform(keys[1], (2, HEADS, 1), jnp.float32, jnp.log(1.0 / 100.0), jnp.log(1.0 / 30.0)))
    rate = jnp.where(slow, 0.3 / TOKENS, fast_rate)
    factor = jnp.exp(jax.random.uniform(keys[2], (2, HEADS, TOKENS // TOK_DEV), jnp.float32, -0.7, 0.7))
    factor = jnp.repeat(factor, TOK_DEV, axis=2)
    noise = jnp.clip(jax.random.normal(keys[3], (2, HEADS, TOKENS), jnp.float32), -3.0, 3.0)
    pre = -jnp.log(rate * factor) + noise
    spots = jax.random.randint(keys[4], (2, HEADS, 3), 0, TOKENS)
    hit = jnp.any(jnp.arange(TOKENS)[None, None, None, :] == spots[..., None], axis=2)
    drop = jax.random.uniform(keys[5], (2, HEADS, TOKENS), jnp.float32, 0.0, 1.4)
    return jnp.where(hit, drop, pre)


def shard_levels(stream_key, extent, cuts, least, high):
    def one(axis_at, shards_of):
        steps = jax.random.uniform(jax.random.fold_in(jax.random.fold_in(stream_key, 6), axis_at), (shards_of,), jnp.float32, least / len(cuts), high / len(cuts))
        return jnp.repeat(jnp.exp(steps), extent[axis_at] // shards_of).reshape((-1,) + (1,) * (len(extent) - axis_at - 1))

    gain = one(*cuts[0])
    for cut in cuts[1:]:
        gain = gain * one(*cut)
    return gain


def profile(amount, total, limit, skew):
    loads = [(1 << 20) // math.isqrt(rank ** skew) + 1 for rank in range(2, amount + 1)]
    rest, holding = total - limit - (amount - 1), [1] * (amount - 1)
    while rest > 0:
        candidates = [i for i in range(amount - 1) if holding[i] < limit]
        pool, budget = sum([loads[i] for i in candidates]), rest
        for i in candidates:
            addition = min(limit - holding[i], max(1, budget * loads[i] // pool), rest)
            holding[i] = holding[i] + addition
            rest = rest - addition
    return np.array([limit] + holding)


def uneven_parts(own_key, count, total, bound, lean):
    if count == 2:
        one = jax.random.randint(own_key, (), max(1, total - bound), min(bound, total - 1) + 1)
        return jnp.stack([one, total - one])
    tallies = jnp.asarray(profile(count, total, bound, lean), jnp.int32)
    pairs = (count - 1) // 2
    source_of, sink = tallies[1:1 + 2 * pairs:2], tallies[2:2 + 2 * pairs:2]
    room = jnp.minimum(source_of - 1, bound - sink)
    moved = jax.random.randint(jax.random.fold_in(own_key, 1), (pairs,), 0, 1 << 20) % (room + 1)
    tallies = tallies.at[1:1 + 2 * pairs:2].set(source_of - moved).at[2:2 + 2 * pairs:2].set(sink + moved)
    return tallies[jax.random.permutation(jax.random.fold_in(own_key, 2), count)]


def gaussian(key, shape, deviation, most, cuts=(), kind=jnp.bfloat16):
    entries = deviation * jax.random.normal(key, shape, jnp.float32)
    if cuts:
        entries = entries * shard_levels(key, shape, cuts, -0.22, 0.18)
    return jnp.clip(entries, -most, most).astype(kind)


def setup_inputs(seed: int = 0) -> dict:
    arg_keys = jax.random.split(jax.random.key(seed), 14)
    queries = gaussian(arg_keys[0], (TOKENS, HEADS * DQK), 1.0, 6.0, ((0, 8), (1, 4)))
    keys = gaussian(arg_keys[1], (TOKENS, HEADS * DQK), 1.0, 6.0, ((0, 8), (1, 4)))
    values = gaussian(arg_keys[2], (TOKENS, HEADS * DV), 1.0, 6.0, ((0, 8), (1, 4)))
    out_gate = gaussian(arg_keys[3], (TOKENS, HEADS * DV), 1.0, 6.0, ((0, 8), (1, 4)))
    input_gates = draw_input_gates(jax.random.fold_in(arg_keys[13], 71), 0)
    forget_gates = draw_forget_gates(jax.random.fold_in(arg_keys[13], 71), 0)
    doc_ids = jnp.searchsorted(jnp.cumsum(uneven_parts(arg_keys[6], N_SP // 2, TOKENS, 4 * TOK_DEV, 0)), jnp.arange(TOKENS), side="right").astype(jnp.int32)
    head_gain = jnp.clip(1.0 + 0.18 * jax.random.normal(arg_keys[7], (HEADS * DV,), jnp.float32), 0.1, 1.9)
    w_out = gaussian(arg_keys[8], (HEADS * DV, D), (HEADS * DV // 4) ** -0.5, 0.25, ((0, 4),))
    resid = draw_resid(jax.random.fold_in(arg_keys[13], 71), 0)
    norm_gain = jnp.clip(1.0 + 0.18 * jax.random.normal(arg_keys[10], (D,), jnp.float32), 0.1, 1.9)
    w_up = gaussian(arg_keys[11], (D, FF), D ** -0.5, 0.125, ((0, 8), (1, 4)))
    w_down = gaussian(arg_keys[12], (FF, D), FF ** -0.5, 0.0625, ((0, 4), (1, 8)))
    return dict(queries=queries, keys=keys, values=values, out_gate=out_gate, input_gates=input_gates, forget_gates=forget_gates, doc_ids=doc_ids, head_gain=head_gain, w_out=w_out, resid=resid, norm_gain=norm_gain, w_up=w_up, w_down=w_down)


eps = 1e-06
far_low = -1e+30

def summarize(keys_blk, values_blk, in_gate, forget_pre, doc_pos):
    logf = jax.nn.log_sigmoid(forget_pre)
    cum = jnp.cumsum(logf)
    length = keys_blk.shape[0]
    last_doc = doc_pos[length - 1]
    tail = doc_pos == last_doc
    total = cum[length - 1]
    exponent = jnp.where(tail, total - cum + in_gate, far_low)
    peak = jnp.max(exponent)
    scaled = jnp.exp(exponent - peak)
    weighted = (keys_blk.astype(jnp.float32) * scaled[:, None]).astype(jnp.bfloat16)
    memory = jnp.einsum('sd,sv->dv', weighted.astype(jnp.float32), values_blk.astype(jnp.float32))
    norm_keys = lax.optimization_barrier(jnp.sum(weighted.astype(jnp.float32), axis=0))
    return (memory, norm_keys, peak, total, doc_pos[0], last_doc, jnp.zeros((), jnp.float32))

def emit(queries_blk, keys_blk, values_blk, in_gate, forget_pre, doc_pos, state):
    memory, norm_keys, top_in, total_in, first_in, last_in, empty_in = state
    scale = queries_blk.shape[1] ** (-0.5)
    logf = jax.nn.log_sigmoid(forget_pre)
    cum = jnp.cumsum(logf)
    length = queries_blk.shape[0]
    place = jnp.arange(length)
    keep = (place[:, None] >= place[None, :]) & (doc_pos[:, None] == doc_pos[None, :])
    exponent = jnp.where(keep, cum[:, None] - cum[None, :] + in_gate[None, :], far_low)
    usable = (doc_pos == last_in) & (empty_in < 0.5)
    carried = jnp.where(usable, cum + top_in, far_low)
    peak = jnp.maximum(carried, lax.optimization_barrier(jnp.max(exponent, axis=1)))
    scores = jnp.einsum('td,sd->ts', queries_blk.astype(jnp.float32), keys_blk.astype(jnp.float32)) * scale
    weights = jnp.where(keep, scores * jnp.exp(exponent - peak[:, None]), 0.0)
    inter = jnp.where(usable, jnp.exp(carried - peak), 0.0)
    query_wide = queries_blk.astype(jnp.float32)
    numer = jnp.dot(weights.astype(jnp.bfloat16), values_blk, preferred_element_type=jnp.float32)
    numer = numer + (inter * scale)[:, None] * jnp.dot(query_wide, memory, precision=lax.Precision.HIGHEST)
    denom = lax.optimization_barrier(jnp.sum(weights, axis=1)) + inter * scale * jnp.dot(query_wide, norm_keys, precision=lax.Precision.HIGHEST)
    return numer / jnp.maximum(jnp.abs(denom), 1.0)[:, None]

def combine(early, late):
    e_mem, e_keys, e_top, e_total, e_first, e_last, e_empty = early
    l_mem, l_keys, l_top, l_total, l_first, l_last, l_empty = late
    linked = (l_first == e_last) & (l_first == l_last) & (e_empty < 0.5)
    top = jnp.where(linked, jnp.maximum(l_top, e_top + l_total), l_top)
    early_part = jnp.where(linked, jnp.exp(jnp.minimum(e_top + l_total - top, 0.0)), 0.0)
    late_part = jnp.exp(l_top - top)
    joined = (early_part * e_mem + late_part * l_mem, early_part * e_keys + late_part * l_keys, top, e_total + l_total, jnp.where(e_empty > 0.5, l_first, e_first), l_last, jnp.zeros_like(l_empty))
    return tuple((jnp.where(l_empty > 0.5, a, b) for a, b in zip(early, joined)))

def run_direction(queries_h, keys_h, values_h, in_gate, forget_pre, doc_pos):

    def blocks(arr):
        return arr.reshape((N_SP, TOK_DEV) + arr.shape[1:])

    def step(state, pieces):
        q_blk, k_blk, v_blk, i_blk, f_blk, d_blk = pieces
        result = emit(q_blk, k_blk, v_blk, i_blk, f_blk, d_blk, state)
        return (combine(state, summarize(k_blk, v_blk, i_blk, f_blk, d_blk)), result)
    start = (jnp.zeros((DQK, DV), jnp.float32), jnp.zeros((DQK,), jnp.float32), jnp.full((), far_low, jnp.float32), jnp.zeros((), jnp.float32), jnp.full((), -1.0, jnp.float32), jnp.full((), -1.0, jnp.float32), jnp.ones((), jnp.float32))
    final, results = lax.scan(step, start, (blocks(queries_h), blocks(keys_h), blocks(values_h), blocks(in_gate), blocks(forget_pre), blocks(doc_pos)))
    return results.reshape(TOKENS, DV)

def reference(queries, keys, values, out_gate, input_gates, forget_gates, doc_ids, head_gain, w_out, resid, norm_gain, w_up, w_down):
    doc_pos = doc_ids.astype(jnp.float32)
    summed = jnp.zeros((TOKENS, D), jnp.float32)
    for head in range(HEADS):
        q_head = queries[:, head * DQK:(head + 1) * DQK]
        k_head = keys[:, head * DQK:(head + 1) * DQK]
        v_head = values[:, head * DV:(head + 1) * DV]
        forward = run_direction(q_head, k_head, v_head, input_gates[0, head], forget_gates[0, head], doc_pos)
        backward = run_direction(q_head[::-1], k_head[::-1], v_head[::-1], input_gates[1, head, ::-1], forget_gates[1, head, ::-1], doc_pos[::-1])[::-1]
        memory = forward + backward
        normed = memory * lax.rsqrt(lax.optimization_barrier(jnp.mean(memory * memory, axis=-1, keepdims=True)) + eps)
        gate = jax.nn.sigmoid(out_gate[:, head * DV:(head + 1) * DV].astype(jnp.float32))
        readout = (normed * head_gain[head * DV:(head + 1) * DV] * gate).astype(jnp.bfloat16)
        part = jnp.dot(readout, w_out[head * DV:(head + 1) * DV], preferred_element_type=jnp.float32).astype(jnp.bfloat16)
        summed = summed + lax.optimization_barrier(part).astype(jnp.float32)
    mixed = resid.astype(jnp.float32) + summed
    scaled = (mixed * lax.rsqrt(lax.optimization_barrier(jnp.mean(mixed * mixed, axis=-1, keepdims=True)) + eps) * norm_gain).astype(jnp.bfloat16)
    width = FF // HEADS

    def feed(rows_blk):
        hidden = jnp.square(jax.nn.relu(jnp.dot(rows_blk, w_up, preferred_element_type=jnp.float32))).astype(jnp.bfloat16)
        total = jnp.zeros((rows_blk.shape[0], D), jnp.float32)
        for group in range(HEADS):
            part = jnp.dot(hidden[:, group * width:(group + 1) * width], w_down[group * width:(group + 1) * width], preferred_element_type=jnp.float32).astype(jnp.bfloat16)
            total = total + lax.optimization_barrier(part).astype(jnp.float32)
        return total
    mixer = lax.map(feed, scaled.reshape(N_SP, TOK_DEV, D)).reshape(TOKENS, D)
    return (mixed + mixer).astype(jnp.bfloat16)
```

```python
import functools

import jax
import jax.numpy as jnp
from jax import lax
from jax.experimental import pallas as pl
from jax.experimental.pallas import tpu as pltpu
from jax.sharding import PartitionSpec as P


eps = 1e-06
far_low = -1e30
longest_doc = 3072


MESH = pl.DeviceIdType.MESH
bf16 = jnp.bfloat16
f32 = jnp.float32


def dot(a, b):
    return jnp.dot(a, b, preferred_element_type=f32)


class Lines:
    def __init__(self):
        count = lax.axis_size("sp")
        self.pair = 2 if count % 2 == 0 else 1
        self.line = count // self.pair

    def along(self, value, step):
        table = [
            (z * self.pair + y, (z + step) * self.pair + y)
            for z in range(self.line)
            for y in range(self.pair)
            if 0 <= z + step < self.line
        ]
        return lax.ppermute(value, "sp", table)

    def across(self, value, valid):
        table = [
            (z * self.pair + y, z * self.pair + 1 - y)
            for z in range(self.line)
            if valid(z)
            for y in range(self.pair)
        ]
        return lax.ppermute(value, "sp", table)

    def order(self):
        place = lax.axis_index("sp")
        z, y = place // self.pair, place % self.pair
        sources = []
        for k in range(self.line):
            row = (z + self.line - k) % self.line
            sources.append(row * self.pair + y)
            if self.pair == 2:
                sources.append(row * self.pair + 1 - y)
        return jnp.stack(sources)

    def piece(self, source):
        place = lax.axis_index("sp")
        z, y = place // self.pair, place % self.pair
        k = (z + self.line - source // self.pair) % self.line
        return k * self.pair + (y + source) % self.pair

    def gather(self, own):
        n = self.line
        up, down = {}, {}
        up_side, down_side = {}, {}
        two = self.pair == 2
        own_side = self.across(own, lambda z: True) if two else None
        prev_up = prev_down = own
        for k in range(1, n):
            prev_up = up[k] = self.along(prev_up, 1)
            prev_down = down[k] = self.along(prev_down, -1)
            if two:
                up_side[k] = self.across(prev_up, lambda z: z >= k)
                down_side[k] = self.across(prev_down, lambda z: z + k < n)
        groups = [[own] + ([own_side] if two else [])]
        z = lax.axis_index("sp") // self.pair
        for k in range(1, n):
            below = z >= k
            group = [jnp.where(below, up[k], down[n - k])]
            if two:
                group.append(jnp.where(below, up_side[k], down_side[n - k]))
            groups.append(group)
        return groups


class Heads:
    def __init__(self):
        count = lax.axis_size("tp")
        self.core = 2 if count % 2 == 0 else 1
        self.far = count // self.core

    def swap(self, value):
        count = lax.axis_size("tp")
        return lax.ppermute(value, "tp", [(i, i ^ 1) for i in range(count)])

    def shift(self, value, step):
        table = [
            (x * self.core + c, ((x + step) % self.far) * self.core + c)
            for x in range(self.far)
            for c in range(self.core)
        ]
        return lax.ppermute(value, "tp", table)

    def gather(self, own):
        mine = [own] + [self.shift(own, r) for r in range(1, self.far)]
        if self.core == 1:
            return jnp.concatenate(mine)
        return jnp.concatenate(mine + [self.swap(block) for block in mine])

    def reduce(self, near, away):
        total = near.astype(f32)
        if away is not None:
            total = total + self.swap(away).astype(f32)
        out = total[0]
        for r in range(1, self.far):
            out = out + self.shift(total[r].astype(bf16), -r).astype(f32)
        return out


def local_part(scores, values, exponent, keep):
    top = jnp.max(jnp.where(keep, exponent, far_low), axis=1)
    weights = jnp.where(keep, scores * jnp.exp(exponent - top[:, None]), 0.0)
    return top, dot(weights.astype(bf16), values), jnp.sum(weights, axis=1)


def summary(keys, exponent):
    peak = jnp.max(exponent)
    weighted = (keys * jnp.exp(exponent - peak)[:, None]).astype(bf16)
    return weighted, jnp.sum(weighted.astype(f32), axis=0), peak


def split_row(row, width):
    terms, rest = [], row
    for _ in range(3):
        term = lax.reduce_precision(rest, 8, 7)
        rest = rest - term
        terms.append(term.astype(bf16))
    lines = -(-row.shape[0] // width)
    table = jnp.stack([jnp.pad(t, (0, lines * width - t.shape[0])) for t in terms])
    table = table.reshape(3 * lines, width)
    return jnp.pad(table, ((0, -(3 * lines) % 16), (0, 0)))


def join_row(table, size):
    lines = -(-size // table.shape[1])
    terms = table[: 3 * lines].astype(f32).reshape(3, -1)
    return (terms[0] + terms[1] + terms[2])[:size]


def incoming(memory, row, doc_here, sign, reach):
    count = lax.axis_size("sp")
    place = lax.axis_index("sp")
    depth, width = memory.shape
    sent = jnp.concatenate([memory, split_row(row, width)])
    arrived = []
    for d in range(1, min(reach, count - 1) + 1):
        table = [(i, i + sign * d) for i in range(count) if 0 <= i + sign * d < count]
        got = lax.ppermute(sent, "sp", table)
        arrived.append((join_row(got[depth:], row.shape[0]), got[:depth]))
    passed = jnp.zeros((), f32)
    levels, linked = [], []
    for d, (got, _) in enumerate(arrived, 1):
        there = (place >= d) if sign > 0 else (place + d < count)
        joined = there & (got[depth + 2] == doc_here)
        levels.append(jnp.where(joined, got[depth] + passed, far_low))
        linked.append(joined)
        passed = passed + got[depth + 1]
    top = jnp.max(jnp.stack(levels))
    state = jnp.zeros(memory.shape, f32)
    norm = jnp.zeros((depth,), f32)
    for level, joined, (got, mem) in zip(levels, linked, arrived):
        share = jnp.where(joined, jnp.exp(level - top), 0.0)
        state = state + share * mem.astype(f32)
        norm = norm + share * got[:depth]
    return state.astype(bf16), norm, top, linked[0]


def one_head(queries, keys, values, in_gates, forget_pre, doc_pos, reach):
    length, depth = queries.shape
    scale = depth ** (-0.5)
    place = jnp.arange(length)
    logf = jax.nn.log_sigmoid(forget_pre)
    before = place[:, None] >= place[None, :]
    after = place[:, None] <= place[None, :]
    cum_f = jnp.sum(jnp.where(before, logf[0][None, :], 0.0), axis=1)
    cum_b = jnp.sum(jnp.where(after, logf[1][None, :], 0.0), axis=1)
    total_f, total_b = cum_f[length - 1], cum_b[0]
    first, last = doc_pos[0], doc_pos[length - 1]
    weighted_f, norm_f, peak_f = summary(
        keys, jnp.where(doc_pos == last, total_f - cum_f + in_gates[0], far_low)
    )
    weighted_b, norm_b, peak_b = summary(
        keys, jnp.where(doc_pos == first, total_b - cum_b + in_gates[1], far_low)
    )

    def own_state(weighted):
        return lax.dot_general(
            weighted, values, (((0,), (0,)), ((), ())), preferred_element_type=f32
        ).astype(bf16)

    pad = jnp.zeros((125,), f32)
    row_f = jnp.concatenate([norm_f, jnp.stack([peak_f, total_f, last]), pad])
    row_b = jnp.concatenate([norm_b, jnp.stack([peak_b, total_b, first]), pad])
    state_f, norm_in_f, top_f, has_f = incoming(own_state(weighted_f), row_f, first, 1, reach)
    state_b, norm_in_b, top_b, has_b = incoming(own_state(weighted_b), row_b, last, -1, reach)

    scores = (
        lax.dot_general(queries, keys, (((1,), (1,)), ((), ())), preferred_element_type=f32) * scale
    )
    same = doc_pos[:, None] == doc_pos[None, :]
    wide = queries.astype(f32)

    def finish(cum, gate, keep, state, norm_in, top_in, usable):
        exponent = cum[:, None] - cum[None, :] + gate[None, :]
        top, numer, denom = local_part(scores, values, exponent, keep)
        carried = jnp.where(usable, cum + top_in, far_low)
        peak = jnp.maximum(carried, top)
        local = jnp.exp(top - peak)
        inter = jnp.where(usable, jnp.exp(carried - peak), 0.0) * scale
        denom = local * denom + inter * jnp.sum(wide * norm_in[None, :], axis=1)
        under = 1.0 / jnp.maximum(jnp.abs(denom), 1.0)
        return (local * under)[:, None] * numer + (inter * under)[:, None] * dot(queries, state)

    return finish(
        cum_f, in_gates[0], before & same, state_f, norm_in_f, top_f, has_f & (doc_pos == first)
    ) + finish(
        cum_b, in_gates[1], after & same, state_b, norm_in_b, top_b, has_b & (doc_pos == last)
    )


def pack(w_up, w_down):
    wide = w_down.shape[1]
    count = w_up.shape[1] // wide
    tiles = [w_down[i * wide : (i + 1) * wide] for i in range(count)]
    return jnp.concatenate([w_up, jnp.concatenate(tiles, axis=1)])


def unpack(table, wide):
    count = table.shape[1] // wide
    return jnp.concatenate([table[:, i * wide : (i + 1) * wide] for i in range(count)])


def shards(*args):
    return layer(*args)


def layer(
    queries,
    keys,
    values,
    out_gate,
    input_gates,
    forget_gates,
    doc_ids,
    head_gain,
    w_out,
    resid,
    norm_gain,
    w_up,
    w_down,
):
    length = queries.shape[0]
    heads = input_gates.shape[1]
    depth, width = queries.shape[1] // heads, values.shape[1] // heads
    lines, tps = Lines(), Heads()
    rows = resid.shape[0]
    doc_pos = doc_ids.astype(f32)
    reach = -(-longest_doc // length)
    deep_up, wide_down = w_up.shape[0], w_down.shape[1]
    groups = lines.gather(pack(w_up, w_down))
    ups = [[piece[:deep_up] for piece in group] for group in groups]
    downs = [[unpack(piece[deep_up:], wide_down) for piece in group] for group in groups]
    order = lines.order()

    parts = []
    for h in range(heads):
        at_k, at_v = slice(h * depth, (h + 1) * depth), slice(h * width, (h + 1) * width)
        memory = one_head(
            queries[:, at_k],
            keys[:, at_k],
            values[:, at_v],
            input_gates[:, h],
            forget_gates[:, h],
            doc_pos,
            reach,
        )
        normed = memory * lax.rsqrt(jnp.mean(memory * memory, axis=-1, keepdims=True) + eps)
        gate = jax.nn.sigmoid(out_gate[:, at_v].astype(f32))
        parts.append((normed * head_gain[at_v] * gate).astype(bf16))
    readout = parts[0] if heads == 1 else jnp.concatenate(parts, axis=1)

    projected = dot(readout, w_out).astype(bf16).reshape(tps.far, tps.core, rows, -1)
    me = lax.axis_index("tp")
    x, c = me // tps.core, me % tps.core

    def for_core(core):
        picked = lax.dynamic_index_in_dim(projected, core, 1, False)
        return jnp.stack(
            [
                lax.dynamic_index_in_dim(picked, (x + tps.far - r) % tps.far, 0, False)
                for r in range(tps.far)
            ]
        )

    summed = tps.reduce(for_core(c), for_core(1 - c) if tps.core == 2 else None)
    mixed = resid.astype(f32) + summed
    factor = lax.rsqrt(jnp.mean(mixed * mixed, axis=-1, keepdims=True) + eps)
    scaled = (mixed * factor * norm_gain).astype(bf16)

    blocks = order.shape[0]
    deep = scaled.shape[1] // blocks
    turned = jnp.concatenate(
        [lax.dynamic_slice_in_dim(scaled, order[i] * deep, deep, 1) for i in range(blocks)], axis=1
    )
    up_full = jnp.concatenate([piece for group in ups for piece in group], axis=0)
    product = dot(tps.gather(turned), up_full)
    hidden = jnp.square(jax.nn.relu(product)).astype(bf16)

    bundle = max(1, len(downs) // 4)
    outs = []
    for at in range(0, len(downs), bundle):
        pieces = [piece for group in downs[at : at + bundle] for piece in group]
        part = dot(hidden, jnp.concatenate(pieces, axis=1)).astype(bf16)
        part = part.reshape(tps.core, tps.far, rows, -1)
        outs.append(tps.reduce(part[0], part[1] if tps.core == 2 else None))
    summed = jnp.concatenate(outs, axis=1)
    back = jnp.concatenate(
        [lax.dynamic_slice_in_dim(summed, lines.piece(i) * deep, deep, 1) for i in range(blocks)],
        axis=1,
    )
    return (mixed + back).astype(bf16)


class Spot:
    def __init__(self, n_sp, n_tp):
        self.n_sp, self.n_tp = n_sp, n_tp
        self.line = n_sp // 2
        self.sp = lax.axis_index("sp")
        self.tp = lax.axis_index("tp")
        self.z, self.y = self.sp // 2, self.sp % 2
        self.x, self.c = self.tp // 2, self.tp % 2
        self.zp = self.z % 2
        self.base = self.z - self.zp

    def at(self, z=None, y=None, x=None, c=None):
        z = self.z if z is None else z
        y = self.y if y is None else y
        x = self.x if x is None else x
        c = self.c if c is None else c
        return (z * 2 + y, x * 2 + c)


class Wire:
    def __init__(self, send_sems, recv_sems):
        self.send_sems, self.recv_sems = send_sems, recv_sems
        self.count = 0

    def slot(self):
        self.count += 1
        return self.count - 1

    def copy(self, src, dst, number, where, arrival=None):
        return pltpu.make_async_remote_copy(
            src_ref=src,
            dst_ref=dst,
            send_sem=self.send_sems.at[number],
            recv_sem=self.recv_sems.at[number if arrival is None else arrival],
            device_id=where,
            device_id_type=MESH,
        )


def layer_kernel(
    n_sp,
    n_tp,
    q_hbm,
    k_hbm,
    v_hbm,
    og_hbm,
    ig_ref,
    fg_ref,
    doc_ref,
    hg_ref,
    wo_hbm,
    res_hbm,
    ng_ref,
    wup_hbm,
    wdn_hbm,
    out_ref,
    q_s,
    k_s,
    v_s,
    og_s,
    wo_s,
    res_s,
    up_s,
    dn_s,
    rows_s,
    cols_s,
    num_s,
    stat_s,
    own_s,
    own_info_s,
    got_s,
    got_info_s,
    mid_s,
    mid_info_s,
    fin_s,
    proj_s,
    fa_s,
    fb_s,
    fc_s,
    fc_in_s,
    mixed_s,
    nrm_s,
    hid_s,
    part_s,
    r1_s,
    r2_out_s,
    r2_keep_s,
    r2_in_s,
    r3_out_s,
    r3_in_s,
    local_sem,
    send_sem,
    recv_sem,
):
    me = Spot(n_sp, n_tp)
    wire = Wire(send_sem, recv_sem)
    line = me.line
    length, depth = q_s.shape
    rows = res_s.shape[0]
    half = rows // 2
    deep = wup_hbm.shape[0]
    hidden = up_s.shape[2]
    wide = wdn_hbm.shape[1]
    scale = depth ** (-0.5)
    waits = []

    def start(copy, cond=None):
        if cond is None:
            copy.start()
            waits.append((copy, None))
        else:
            pl.when(cond)(copy.start)
            waits.append((copy, cond))

    def load(src, dst, number):
        copy = pltpu.make_async_copy(src, dst, local_sem.at[number])
        copy.start()
        return copy

    up_z = [wire.slot() for _ in range(line)][0]
    dn_z = [wire.slot() for _ in range(line)][0]
    up_y = [wire.slot() for _ in range(line)][0]
    dn_y = [wire.slot() for _ in range(line)][0]

    planes = [me.z, me.base + 1 - me.zp] + [lax.rem(me.base + i, line) for i in range(2, line)]

    def up_piece(z):
        return wup_hbm.at[:, pl.ds(pl.multiple_of((z % 2) * hidden, hidden), hidden)]

    def dn_piece(z):
        return wdn_hbm.at[pl.ds(pl.multiple_of((z % 2) * hidden, hidden), hidden), :]

    def send_up(i):
        z = planes[i]
        start(wire.copy(up_piece(z), up_s.at[me.sp], up_z + z, me.at(z=z), up_z + me.z))

    def send_dn(i):
        z = planes[i]
        start(wire.copy(dn_piece(z), dn_s.at[me.sp], dn_z + z, me.at(z=z), dn_z + me.z))

    def recv_up(z):
        wire.copy(up_piece(z), up_s.at[z * 2 + me.y], up_z + z, me.at(z=z)).wait_recv()

    def recv_dn(z):
        wire.copy(dn_piece(z), dn_s.at[z * 2 + me.y], dn_z + z, me.at(z=z)).wait_recv()

    def cross_up(z, src=None):
        slot = z * 2 + me.y
        src = up_s.at[slot] if src is None else src
        start(wire.copy(src, up_s.at[slot], up_y + z, me.at(y=1 - me.y)))

    def cross_dn(z, src=None):
        slot = z * 2 + me.y
        src = dn_s.at[slot] if src is None else src
        start(wire.copy(src, dn_s.at[slot], dn_y + z, me.at(y=1 - me.y)))

    def crossed_up(z):
        slot = z * 2 + 1 - me.y
        wire.copy(up_s.at[slot], up_s.at[slot], up_y + z, me.at(y=1 - me.y)).wait_recv()

    def crossed_dn(z):
        slot = z * 2 + 1 - me.y
        wire.copy(dn_s.at[slot], dn_s.at[slot], dn_y + z, me.at(y=1 - me.y)).wait_recv()

    for i in range(2, line):
        send_up(i)
    cross_up(me.z, up_piece(me.z))
    k_in = load(k_hbm, k_s, 0)
    v_in = load(v_hbm, v_s, 1)
    q_in = load(q_hbm, q_s, 2)
    og_in = load(og_hbm, og_s, 3)
    wo_in = load(wo_hbm, wo_s, 4)
    res_in = load(res_hbm, res_s, 5)
    up_in = load(up_piece(me.z), up_s.at[me.sp], 6)
    dn_in = load(dn_piece(me.z), dn_s.at[me.sp], 7)

    lane = lax.broadcasted_iota(jnp.int32, (8, length), 1)
    sub = lax.broadcasted_iota(jnp.int32, (8, length), 0)
    pre = fg_ref[...]
    logf = jnp.minimum(pre, 0.0) - jnp.log1p(jnp.exp(-jnp.abs(pre)))
    cum_f = jnp.broadcast_to(logf[0:1], (8, length))
    cum_b = jnp.broadcast_to(logf[1:2], (8, length))
    step = 1
    while step < length:
        cum_f = cum_f + jnp.where(lane >= step, pltpu.roll(cum_f, step, 1), 0.0)
        cum_b = cum_b + jnp.where(lane < length - step, pltpu.roll(cum_b, length - step, 1), 0.0)
        step *= 2
    gate = ig_ref[...]
    rel_f = jnp.broadcast_to(gate[0:1], (8, length)) - cum_f
    rel_b = jnp.broadcast_to(gate[1:2], (8, length)) - cum_b
    doc = jnp.broadcast_to(doc_ref[...].astype(f32), (8, length))
    total_f, total_b = cum_f[:, length - 1 :], cum_b[:, 0:1]
    first, last = doc[:, 0:1], doc[:, length - 1 :]
    exp_f = jnp.where(doc == last, total_f + rel_f, far_low)
    exp_b = jnp.where(doc == first, total_b + rel_b, far_low)
    peak_f = jnp.max(exp_f, axis=1, keepdims=True)
    peak_b = jnp.max(exp_b, axis=1, keepdims=True)
    keep_f, keep_b = jnp.exp(exp_f - peak_f), jnp.exp(exp_b - peak_b)
    rows_s[...] = jnp.where(sub == 0, rel_f, jnp.where(sub == 1, rel_b, doc))
    table = jnp.where(sub == 0, cum_f, cum_b)
    table = jnp.where(sub == 2, doc, table)
    table = jnp.where(sub == 3, keep_f, table)
    table = jnp.where(sub == 4, keep_b, table)
    cols_s[...] = table.T

    k_in.wait()
    v_in.wait()
    wide_keys = k_s[...].astype(f32)

    def own(d, column, peak, total, doc_out):
        weighted = (wide_keys * cols_s[:, column : column + 1]).astype(bf16)
        norm = jnp.sum(weighted.astype(f32), axis=0, keepdims=True)
        own_s[d] = lax.dot_general(
            weighted, v_s[...], (((0,), (0,)), ((), ())), preferred_element_type=f32
        ).astype(bf16)
        at = lax.broadcasted_iota(jnp.int32, (8, depth), 0)
        info = jnp.where(at == 0, jnp.broadcast_to(norm, (8, depth)), peak)
        info = jnp.where(at == 2, total, info)
        own_info_s[d] = jnp.where(at == 3, doc_out, info)

    own(0, 3, peak_f, total_f, last)
    own(1, 4, peak_b, total_b, first)

    def reach_of(d, far):
        sign = 1 if d == 0 else -1
        to, frm = me.sp + sign * far, me.sp - sign * far
        can_send = (to < n_sp) if d == 0 else (to >= 0)
        can_recv = (frm >= 0) if d == 0 else (frm < n_sp)
        return to, can_send, can_recv

    state_no = [[(wire.slot(), wire.slot()) for _ in range(2)] for _ in range(3)]

    def state_copies(r, d, far, src, info):
        to, can_send, can_recv = reach_of(d, far)
        to = jnp.clip(to, 0, n_sp - 1)
        a, b = state_no[r][d]
        return (
            wire.copy(src.at[d], got_s.at[r, d], a, (to, me.tp)),
            wire.copy(info.at[d], got_info_s.at[r, d], b, (to, me.tp)),
            can_send,
            can_recv,
        )

    def state_send(r, d, far, src, info):
        mem, note, can_send, can_recv = state_copies(r, d, far, src, info)
        start(note, can_send)
        start(mem, can_send)

        @pl.when(jnp.logical_not(can_recv))
        def _():
            got_s[r, d] = jnp.zeros(got_s.shape[2:], bf16)
            got_info_s[r, d] = jnp.full(got_info_s.shape[2:], -1.0, f32)

    def state_recv(r, d, far, src, info):
        mem, note, _, can_recv = state_copies(r, d, far, src, info)

        @pl.when(can_recv)
        def _():
            note.wait_recv()
            mem.wait_recv()

    for far in (1, 2):
        for d in (0, 1):
            state_send(far - 1, d, far, own_s, own_info_s)
    send_up(1)

    q_in.wait()

    def inside(j, carry):
        r0 = pl.multiple_of(j * rows, rows)
        score = (
            lax.dot_general(
                q_s[pl.ds(r0, rows), :],
                k_s[...],
                (((1,), (1,)), ((), ())),
                preferred_element_type=f32,
            )
            * scale
        )
        at_row = lax.broadcasted_iota(jnp.int32, (rows, length), 0) + r0
        at_col = lax.broadcasted_iota(jnp.int32, (rows, length), 1)
        cols = cols_s[pl.ds(r0, rows), :]
        same = cols[:, 2:3] == rows_s[2:3, :]
        for d in (0, 1):
            order = (at_row >= at_col) if d == 0 else (at_row <= at_col)
            exponent = jnp.where(
                same & order, cols[:, d : d + 1] + rows_s[d : d + 1, :], far_low
            )
            top = jnp.max(exponent, axis=1, keepdims=True)
            weights = score * jnp.exp(exponent - top)
            stat_s[2 * d, pl.ds(r0, rows), :] = top
            stat_s[2 * d + 1, pl.ds(r0, rows), :] = jnp.sum(weights, axis=1, keepdims=True)
            num_s[d, pl.ds(r0, rows), :] = jnp.dot(
                weights.astype(bf16), v_s[...], preferred_element_type=f32
            )
        return carry

    lax.fori_loop(0, length // rows, inside, 0)

    def info_row(r, d, i):
        return got_info_s[r, d, i : i + 1, :]

    near = []
    for d in (0, 1):
        here = (first if d == 0 else last)[0:1]
        state_recv(0, d, 1, own_s, own_info_s)
        state_recv(1, d, 2, own_s, own_info_s)
        link1 = info_row(0, d, 3) == here
        link2 = info_row(1, d, 3) == here
        level1 = jnp.where(link1, info_row(0, d, 1), far_low)
        level2 = jnp.where(link2, info_row(1, d, 1) + info_row(0, d, 2), far_low)
        top = jnp.maximum(level1, level2)
        share1 = jnp.where(link1, jnp.exp(level1 - top), 0.0)
        share2 = jnp.where(link2, jnp.exp(level2 - top), 0.0)
        norm = share1 * info_row(0, d, 0) + share2 * info_row(1, d, 0)
        mid_s[d] = (
            share1[:, 0:1] * got_s[0, d].astype(f32) + share2[:, 0:1] * got_s[1, d].astype(f32)
        ).astype(bf16)
        at = lax.broadcasted_iota(jnp.int32, (8, depth), 0)
        mid_info_s[d] = jnp.where(at == 0, norm, jnp.where(at == 1, top, here))
        state_send(2, d, 2, mid_s, mid_info_s)
        near.append((here, top, norm))

    for i in range(2, line):
        recv_up(planes[i])
        cross_up(planes[i])
    recv_up(planes[1])
    cross_up(planes[1])

    ends = []
    for d in (0, 1):
        here, top, norm = near[d]
        state_recv(2, d, 2, mid_s, mid_info_s)
        link = info_row(2, d, 3) == here
        level = jnp.where(
            link, info_row(2, d, 1) + info_row(1, d, 2) + info_row(0, d, 2), far_low
        )
        peak = jnp.maximum(top, level)
        link1 = info_row(0, d, 3) == here
        share = jnp.where(link1, jnp.exp(top - peak), 0.0)
        share_far = jnp.where(link, jnp.exp(level - peak), 0.0)
        fin_s[d] = (
            share[:, 0:1] * mid_s[d].astype(f32) + share_far[:, 0:1] * got_s[2, d].astype(f32)
        ).astype(bf16)
        meets = jnp.where(link1, here, -2.0)
        ends.append((meets[:, 0:1], peak, share * norm + share_far * info_row(2, d, 0)))

    og_in.wait()
    wo_in.wait()

    def project(j, store):
        r0 = pl.multiple_of(j * rows, rows)
        queries = q_s[pl.ds(r0, rows), :]
        wide_q = queries.astype(f32)
        cols = cols_s[pl.ds(r0, rows), :]
        memory = None
        for d in (0, 1):
            meets, level, norm = ends[d]
            usable = cols[:, 2:3] == meets
            carried = jnp.where(usable, cols[:, d : d + 1] + level[:, 0:1], far_low)
            top = stat_s[2 * d, pl.ds(r0, rows), :]
            peak = jnp.maximum(carried, top)
            local = jnp.exp(top - peak)
            inter = jnp.where(usable, jnp.exp(carried - peak), 0.0) * scale
            den = local * stat_s[2 * d + 1, pl.ds(r0, rows), :] + inter * jnp.sum(
                wide_q * norm, axis=1, keepdims=True
            )
            under = 1.0 / jnp.maximum(jnp.abs(den), 1.0)
            term = (local * under) * num_s[d, pl.ds(r0, rows), :] + (inter * under) * jnp.dot(
                queries, fin_s[d], preferred_element_type=f32
            )
            memory = term if memory is None else memory + term
        normed = memory * lax.rsqrt(jnp.mean(memory * memory, axis=1, keepdims=True) + eps)
        open_gate = jax.nn.sigmoid(og_s[pl.ds(r0, rows), :].astype(f32))
        readout = (normed * hg_ref[...] * open_gate).astype(bf16)
        store(jnp.dot(readout, wo_s[...], preferred_element_type=f32))

    fa_no, fb_no, fc_no = wire.slot(), wire.slot(), wire.slot()
    core = me.at(c=1 - me.c)
    over = me.at(x=1 - me.x)
    above = me.at(z=me.base + 1 - me.zp)
    far_x, far_c = 1 - me.x, 1 - me.c

    def put(ref):
        def store(value):
            ref[...] = value.astype(ref.dtype)

        return store

    fa = wire.copy(proj_s.at[0], fa_s, fa_no, core)
    fb = wire.copy(proj_s.at[2], fb_s, fb_no, core)
    fc = wire.copy(fc_s, fc_in_s, fc_no, over)
    project(far_x * 2 + far_c, put(proj_s.at[0]))
    start(fa)
    project(far_x * 2 + me.c, put(proj_s.at[1]))
    fa.wait_recv()
    fc_s[...] = (proj_s[1].astype(f32) + fa_s[...].astype(f32)).astype(bf16)
    start(fc)
    project(me.x * 2 + far_c, put(proj_s.at[2]))
    start(fb)
    project(me.x * 2 + me.c, put(proj_s.at[3]))
    res_in.wait()
    fb.wait_recv()
    near_sum = res_s[...].astype(f32) + proj_s[3].astype(f32) + fb_s[...].astype(f32)
    mixed_s[...] = near_sum
    fc.wait_recv()
    mixed = mixed_s[...] + fc_in_s[...].astype(f32)
    mixed_s[...] = mixed
    factor = lax.rsqrt(jnp.mean(mixed * mixed, axis=1, keepdims=True) + eps)
    mine = me.zp * n_tp + me.tp
    nrm_s[mine] = (mixed * factor * ng_ref[...]).astype(bf16)

    def owner(zp, x, c):
        return zp * n_tp + x * 2 + c

    far_z = 1 - me.zp
    n_core = [wire.slot() for _ in range(5)]
    n_x, n_z, n_xh, n_zh = wire.slot(), wire.slot(), wire.slot(), wire.slot()
    top_half, low_half = pl.ds(0, half), pl.ds(half, half)

    def pass_on(number, where, who, part=None):
        ref = nrm_s.at[who] if part is None else nrm_s.at[who, part]
        return wire.copy(ref, ref, number, where)

    start(pass_on(n_x, over, mine))
    start(pass_on(n_z, above, mine))
    start(pass_on(n_core[0], core, mine))
    for i in range(2, line):
        send_dn(i)
    send_dn(1)
    cross_dn(me.z, dn_piece(me.z))

    up_in.wait()
    for z in planes:
        crossed_up(z)

    def raise_rows(zp, x):
        group = zp * 2 + x

        def chunk(n, carry):
            c0 = pl.multiple_of(n * 256, 256)
            left = nrm_s[pl.ds(group * 2, 2), :, :].reshape(2 * rows, nrm_s.shape[2])
            right = up_s[:, :, pl.ds(c0, 256)].reshape(n_sp * deep, 256)
            pre = jnp.maximum(jnp.dot(left, right, preferred_element_type=f32), 0.0)
            hid_s[group, :, pl.ds(c0, 256)] = (pre * pre).astype(bf16)
            return carry

        lax.fori_loop(0, hidden // 256, chunk, 0)

    pass_on(n_core[0], core, owner(me.zp, me.x, far_c)).wait_recv()
    raise_rows(me.zp, me.x)
    who = owner(me.zp, far_x, me.c)
    pass_on(n_x, over, who).wait_recv()
    start(pass_on(n_zh, above, who, top_half))
    start(pass_on(n_core[1], core, who))
    who = owner(far_z, me.x, me.c)
    pass_on(n_z, above, who).wait_recv()
    start(pass_on(n_xh, over, who, low_half))
    start(pass_on(n_core[2], core, who))
    pass_on(n_core[1], core, owner(me.zp, far_x, far_c)).wait_recv()
    raise_rows(me.zp, far_x)
    pass_on(n_core[2], core, owner(far_z, me.x, far_c)).wait_recv()
    raise_rows(far_z, me.x)
    who = owner(far_z, far_x, me.c)
    pass_on(n_zh, above, who, top_half).wait_recv()
    start(pass_on(n_core[3], core, who, top_half))
    pass_on(n_xh, over, who, low_half).wait_recv()
    start(pass_on(n_core[4], core, who, low_half))
    who = owner(far_z, far_x, far_c)
    pass_on(n_core[3], core, who, top_half).wait_recv()
    pass_on(n_core[4], core, who, low_half).wait_recv()
    raise_rows(far_z, far_x)

    blocks = n_sp
    order = []
    for i in range(line):
        z = lax.rem(me.base + i, line)
        order += [(z, me.y), (z, 1 - me.y)]
    r1_no = [wire.slot() for _ in range(blocks)]
    r2_no = [wire.slot() for _ in range(blocks)]
    r3_no = [wire.slot() for _ in range(blocks)]
    groups = 4

    def pump(i):
        z = lax.rem(me.base + i, line)

        @pl.when(z == me.z)
        def _():
            dn_in.wait()

        if i < 2:

            @pl.when(z != me.z)
            def _():
                recv_dn(z)
                wire.copy(
                    dn_s.at[z * 2 + me.y], dn_s.at[z * 2 + me.y], dn_y + z, me.at(y=1 - me.y)
                ).start()

            waits.append(
                (
                    wire.copy(
                        dn_s.at[z * 2 + me.y], dn_s.at[z * 2 + me.y], dn_y + z, me.at(y=1 - me.y)
                    ),
                    z != me.z,
                )
            )
        else:
            recv_dn(z)
            cross_dn(z)

    def lower(k):
        z, y = order[k]
        if k % 2 == 0:
            if k == 0:
                pump(0)
            if k // 2 + 1 < line:
                pump(k // 2 + 1)
        else:
            crossed_dn(z)
        slot = z * 2 + y

        def one(g, carry):
            value = jnp.dot(hid_s[g], dn_s[slot], preferred_element_type=f32).astype(bf16)
            part_s[k, 0, g] = value[:rows]
            part_s[k, 1, g] = value[rows:]
            return carry

        lax.fori_loop(0, groups, one, 0)
        start(wire.copy(part_s.at[k, far_c], r1_s.at[k], r1_no[k], core))

    def sum1(k):
        wire.copy(part_s.at[k, far_c], r1_s.at[k], r1_no[k], core).wait_recv()

        def both(g):
            return part_s[k, me.c, g].astype(f32) + r1_s[k, g].astype(f32)

        for i in range(2):
            away = i * 2 + far_x if k % 2 == 0 else far_z * 2 + i
            r2_out_s[k, i] = both(away).astype(bf16)
        start(wire.copy(r2_out_s.at[k], r2_in_s.at[k], r2_no[k], over if k % 2 == 0 else above))
        for i in range(2):
            here = i * 2 + me.x if k % 2 == 0 else me.zp * 2 + i
            r2_keep_s[k, i] = both(here)

    def sum2(k):
        wire.copy(
            r2_out_s.at[k], r2_in_s.at[k], r2_no[k], over if k % 2 == 0 else above
        ).wait_recv()
        far = far_z if k % 2 == 0 else far_x
        r3_out_s[k] = (r2_keep_s[k, far] + r2_in_s[k, far].astype(f32)).astype(bf16)
        start(wire.copy(r3_out_s.at[k], r3_in_s.at[k], r3_no[k], above if k % 2 == 0 else over))

    def sum3(k):
        wire.copy(
            r3_out_s.at[k], r3_in_s.at[k], r3_no[k], above if k % 2 == 0 else over
        ).wait_recv()
        z, y = order[k]
        c0 = pl.multiple_of((z * 2 + y) * wide, wide)
        at = me.zp if k % 2 == 0 else me.x
        total = r2_keep_s[k, at] + r2_in_s[k, at].astype(f32) + r3_in_s[k].astype(f32)
        total = mixed_s[:, pl.ds(c0, wide)] + total
        out_ref[:, pl.ds(c0, wide)] = total.astype(bf16)

    for k in range(blocks + 3):
        if k < blocks:
            lower(k)
        if 0 <= k - 1 < blocks:
            sum1(k - 1)
        if 0 <= k - 2 < blocks:
            sum2(k - 2)
        if 0 <= k - 3 < blocks:
            sum3(k - 3)

    for copy, cond in waits:
        if cond is None:
            copy.wait_send()
        else:
            pl.when(cond)(copy.wait_send)


def fused(n_sp, n_tp, *args):
    (
        queries,
        keys,
        values,
        out_gate,
        input_gates,
        forget_gates,
        doc_ids,
        head_gain,
        w_out,
        resid,
        norm_gain,
        w_up,
        w_down,
    ) = args
    length, depth = queries.shape
    width = values.shape[1]
    rows, model = resid.shape
    deep, wide = w_up.shape[0], w_down.shape[1]
    hidden = w_up.shape[1] // 2
    line = n_sp // 2
    blocks = n_sp
    numbers = 4 * line + 24 + 3 * blocks
    vmem = pltpu.VMEM
    scratch = [
        vmem((length, depth), bf16),
        vmem((length, depth), bf16),
        vmem((length, width), bf16),
        vmem((length, width), bf16),
        vmem((width, model), bf16),
        vmem((rows, model), bf16),
        vmem((n_sp, deep, hidden), bf16),
        vmem((n_sp, hidden, wide), bf16),
        vmem((8, length), f32),
        vmem((length, 8), f32),
        vmem((2, length, width), f32),
        vmem((4, length, 1), f32),
        vmem((2, depth, width), bf16),
        vmem((2, 8, depth), f32),
        vmem((3, 2, depth, width), bf16),
        vmem((3, 2, 8, depth), f32),
        vmem((2, depth, width), bf16),
        vmem((2, 8, depth), f32),
        vmem((2, depth, width), bf16),
        vmem((4, rows, model), bf16),
        vmem((rows, model), bf16),
        vmem((rows, model), bf16),
        vmem((rows, model), bf16),
        vmem((rows, model), bf16),
        vmem((rows, model), f32),
        vmem((2 * n_tp, rows, model), bf16),
        vmem((4, 2 * rows, hidden), bf16),
        vmem((blocks, 2, 4, rows, wide), bf16),
        vmem((blocks, 4, rows, wide), bf16),
        vmem((blocks, 2, rows, wide), bf16),
        vmem((blocks, 2, rows, wide), f32),
        vmem((blocks, 2, rows, wide), bf16),
        vmem((blocks, rows, wide), bf16),
        vmem((blocks, rows, wide), bf16),
        pltpu.SemaphoreType.DMA((8,)),
        pltpu.SemaphoreType.DMA((numbers,)),
        pltpu.SemaphoreType.DMA((numbers,)),
    ]
    anywhere = pl.BlockSpec(memory_space=pl.ANY)
    inside = pl.BlockSpec(memory_space=pltpu.VMEM)
    return pl.pallas_call(
        functools.partial(layer_kernel, n_sp, n_tp),
        out_shape=jax.ShapeDtypeStruct((rows, model), bf16),
        in_specs=[anywhere] * 4 + [inside] * 4 + [anywhere] * 2 + [inside] + [anywhere] * 2,
        out_specs=inside,
        scratch_shapes=scratch,
        compiler_params=pltpu.CompilerParams(has_side_effects=True, vmem_limit_bytes=66_000_000),
        name="layer",
    )(
        queries,
        keys,
        values,
        out_gate,
        input_gates.reshape(2, length),
        forget_gates.reshape(2, length),
        doc_ids.reshape(1, length),
        head_gain.reshape(1, width),
        w_out,
        resid,
        norm_gain.reshape(1, model),
        w_up,
        w_down,
    )


def fits(mesh, args):
    n_sp, n_tp = mesh.shape["sp"], mesh.shape["tp"]
    queries, input_gates, w_up, w_down = args[0], args[4], args[11], args[12]
    length = queries.shape[0] // n_sp
    return (
        n_tp == 4
        and n_sp % 4 == 0
        and input_gates.shape[1] == n_tp
        and -(-longest_doc // length) <= 4
        and length % (n_tp * 32) == 0
        and w_down.shape[1] % (n_sp * 128) == 0
        and w_up.shape[0] % (n_sp * 16) == 0
        and w_up.shape[1] % (n_tp * 512) == 0
    )


def solution(mesh):
    in_specs = (
        P("sp", "tp"),
        P("sp", "tp"),
        P("sp", "tp"),
        P("sp", "tp"),
        P(None, "tp", "sp"),
        P(None, "tp", "sp"),
        P("sp"),
        P("tp"),
        P("tp", None),
        P(("sp", "tp"), None),
        P(),
        P("sp", "tp"),
        P("tp", "sp"),
    )
    out_specs = P(("sp", "tp"), None)

    def step(*args):
        whole = fits(mesh, args)
        body = functools.partial(fused, mesh.shape["sp"], mesh.shape["tp"]) if whole else shards
        return jax.shard_map(
            body, mesh=mesh, in_specs=in_specs, out_specs=out_specs, check_vma=False
        )(*args)

    return step
```

```python
import functools

import jax
import jax.numpy as jnp
from jax import lax
from jax.experimental import pallas as pl
from jax.experimental.pallas import tpu as pltpu
from jax.sharding import PartitionSpec as P


eps = 1e-06
far_low = -1e30
longest_doc = 3072


MESH = pl.DeviceIdType.MESH
bf16 = jnp.bfloat16
f32 = jnp.float32


def dot(a, b):
    return jnp.dot(a, b, preferred_element_type=f32)


class Lines:
    def __init__(self):
        count = lax.axis_size("sp")
        self.pair = 2 if count % 2 == 0 else 1
        self.line = count // self.pair

    def along(self, value, step):
        table = [
            (z * self.pair + y, (z + step) * self.pair + y)
            for z in range(self.line)
            for y in range(self.pair)
            if 0 <= z + step < self.line
        ]
        return lax.ppermute(value, "sp", table)

    def across(self, value, valid):
        table = [
            (z * self.pair + y, z * self.pair + 1 - y)
            for z in range(self.line)
            if valid(z)
            for y in range(self.pair)
        ]
        return lax.ppermute(value, "sp", table)

    def order(self):
        place = lax.axis_index("sp")
        z, y = place // self.pair, place % self.pair
        sources = []
        for k in range(self.line):
            row = (z + self.line - k) % self.line
            sources.append(row * self.pair + y)
            if self.pair == 2:
                sources.append(row * self.pair + 1 - y)
        return jnp.stack(sources)

    def piece(self, source):
        place = lax.axis_index("sp")
        z, y = place // self.pair, place % self.pair
        k = (z + self.line - source // self.pair) % self.line
        return k * self.pair + (y + source) % self.pair

    def gather(self, own):
        n = self.line
        up, down = {}, {}
        up_side, down_side = {}, {}
        two = self.pair == 2
        own_side = self.across(own, lambda z: True) if two else None
        prev_up = prev_down = own
        for k in range(1, n):
            prev_up = up[k] = self.along(prev_up, 1)
            prev_down = down[k] = self.along(prev_down, -1)
            if two:
                up_side[k] = self.across(prev_up, lambda z: z >= k)
                down_side[k] = self.across(prev_down, lambda z: z + k < n)
        groups = [[own] + ([own_side] if two else [])]
        z = lax.axis_index("sp") // self.pair
        for k in range(1, n):
            below = z >= k
            group = [jnp.where(below, up[k], down[n - k])]
            if two:
                group.append(jnp.where(below, up_side[k], down_side[n - k]))
            groups.append(group)
        return groups


class Heads:
    def __init__(self):
        count = lax.axis_size("tp")
        self.core = 2 if count % 2 == 0 else 1
        self.far = count // self.core

    def swap(self, value):
        count = lax.axis_size("tp")
        return lax.ppermute(value, "tp", [(i, i ^ 1) for i in range(count)])

    def shift(self, value, step):
        table = [
            (x * self.core + c, ((x + step) % self.far) * self.core + c)
            for x in range(self.far)
            for c in range(self.core)
        ]
        return lax.ppermute(value, "tp", table)

    def gather(self, own):
        mine = [own] + [self.shift(own, r) for r in range(1, self.far)]
        if self.core == 1:
            return jnp.concatenate(mine)
        return jnp.concatenate(mine + [self.swap(block) for block in mine])

    def reduce(self, near, away):
        total = near.astype(f32)
        if away is not None:
            total = total + self.swap(away).astype(f32)
        out = total[0]
        for r in range(1, self.far):
            out = out + self.shift(total[r].astype(bf16), -r).astype(f32)
        return out


def local_part(scores, values, exponent, keep):
    top = jnp.max(jnp.where(keep, exponent, far_low), axis=1)
    weights = jnp.where(keep, scores * jnp.exp(exponent - top[:, None]), 0.0)
    return top, dot(weights.astype(bf16), values), jnp.sum(weights, axis=1)


def summary(keys, exponent):
    peak = jnp.max(exponent)
    weighted = (keys * jnp.exp(exponent - peak)[:, None]).astype(bf16)
    return weighted, jnp.sum(weighted.astype(f32), axis=0), peak


def split_row(row, width):
    terms, rest = [], row
    for _ in range(3):
        term = lax.reduce_precision(rest, 8, 7)
        rest = rest - term
        terms.append(term.astype(bf16))
    lines = -(-row.shape[0] // width)
    table = jnp.stack([jnp.pad(t, (0, lines * width - t.shape[0])) for t in terms])
    table = table.reshape(3 * lines, width)
    return jnp.pad(table, ((0, -(3 * lines) % 16), (0, 0)))


def join_row(table, size):
    lines = -(-size // table.shape[1])
    terms = table[: 3 * lines].astype(f32).reshape(3, -1)
    return (terms[0] + terms[1] + terms[2])[:size]


def incoming(memory, row, doc_here, sign, reach):
    count = lax.axis_size("sp")
    place = lax.axis_index("sp")
    depth, width = memory.shape
    sent = jnp.concatenate([memory, split_row(row, width)])
    arrived = []
    for d in range(1, min(reach, count - 1) + 1):
        table = [(i, i + sign * d) for i in range(count) if 0 <= i + sign * d < count]
        got = lax.ppermute(sent, "sp", table)
        arrived.append((join_row(got[depth:], row.shape[0]), got[:depth]))
    passed = jnp.zeros((), f32)
    levels, linked = [], []
    for d, (got, _) in enumerate(arrived, 1):
        there = (place >= d) if sign > 0 else (place + d < count)
        joined = there & (got[depth + 2] == doc_here)
        levels.append(jnp.where(joined, got[depth] + passed, far_low))
        linked.append(joined)
        passed = passed + got[depth + 1]
    top = jnp.max(jnp.stack(levels))
    state = jnp.zeros(memory.shape, f32)
    norm = jnp.zeros((depth,), f32)
    for level, joined, (got, mem) in zip(levels, linked, arrived):
        share = jnp.where(joined, jnp.exp(level - top), 0.0)
        state = state + share * mem.astype(f32)
        norm = norm + share * got[:depth]
    return state.astype(bf16), norm, top, linked[0]


def one_head(queries, keys, values, in_gates, forget_pre, doc_pos, reach):
    length, depth = queries.shape
    scale = depth ** (-0.5)
    place = jnp.arange(length)
    logf = jax.nn.log_sigmoid(forget_pre)
    before = place[:, None] >= place[None, :]
    after = place[:, None] <= place[None, :]
    cum_f = jnp.sum(jnp.where(before, logf[0][None, :], 0.0), axis=1)
    cum_b = jnp.sum(jnp.where(after, logf[1][None, :], 0.0), axis=1)
    total_f, total_b = cum_f[length - 1], cum_b[0]
    first, last = doc_pos[0], doc_pos[length - 1]
    weighted_f, norm_f, peak_f = summary(
        keys, jnp.where(doc_pos == last, total_f - cum_f + in_gates[0], far_low)
    )
    weighted_b, norm_b, peak_b = summary(
        keys, jnp.where(doc_pos == first, total_b - cum_b + in_gates[1], far_low)
    )

    def own_state(weighted):
        return lax.dot_general(
            weighted, values, (((0,), (0,)), ((), ())), preferred_element_type=f32
        ).astype(bf16)

    pad = jnp.zeros((125,), f32)
    row_f = jnp.concatenate([norm_f, jnp.stack([peak_f, total_f, last]), pad])
    row_b = jnp.concatenate([norm_b, jnp.stack([peak_b, total_b, first]), pad])
    state_f, norm_in_f, top_f, has_f = incoming(own_state(weighted_f), row_f, first, 1, reach)
    state_b, norm_in_b, top_b, has_b = incoming(own_state(weighted_b), row_b, last, -1, reach)

    scores = (
        lax.dot_general(queries, keys, (((1,), (1,)), ((), ())), preferred_element_type=f32) * scale
    )
    same = doc_pos[:, None] == doc_pos[None, :]
    wide = queries.astype(f32)

    def finish(cum, gate, keep, state, norm_in, top_in, usable):
        exponent = cum[:, None] - cum[None, :] + gate[None, :]
        top, numer, denom = local_part(scores, values, exponent, keep)
        carried = jnp.where(usable, cum + top_in, far_low)
        peak = jnp.maximum(carried, top)
        local = jnp.exp(top - peak)
        inter = jnp.where(usable, jnp.exp(carried - peak), 0.0) * scale
        denom = local * denom + inter * jnp.sum(wide * norm_in[None, :], axis=1)
        under = 1.0 / jnp.maximum(jnp.abs(denom), 1.0)
        return (local * under)[:, None] * numer + (inter * under)[:, None] * dot(queries, state)

    return finish(
        cum_f, in_gates[0], before & same, state_f, norm_in_f, top_f, has_f & (doc_pos == first)
    ) + finish(
        cum_b, in_gates[1], after & same, state_b, norm_in_b, top_b, has_b & (doc_pos == last)
    )


def pack(w_up, w_down):
    wide = w_down.shape[1]
    count = w_up.shape[1] // wide
    tiles = [w_down[i * wide : (i + 1) * wide] for i in range(count)]
    return jnp.concatenate([w_up, jnp.concatenate(tiles, axis=1)])


def unpack(table, wide):
    count = table.shape[1] // wide
    return jnp.concatenate([table[:, i * wide : (i + 1) * wide] for i in range(count)])


def shards(*args):
    return layer(*args)


def layer(
    queries,
    keys,
    values,
    out_gate,
    input_gates,
    forget_gates,
    doc_ids,
    head_gain,
    w_out,
    resid,
    norm_gain,
    w_up,
    w_down,
):
    length = queries.shape[0]
    heads = input_gates.shape[1]
    depth, width = queries.shape[1] // heads, values.shape[1] // heads
    lines, tps = Lines(), Heads()
    rows = resid.shape[0]
    doc_pos = doc_ids.astype(f32)
    reach = -(-longest_doc // length)
    deep_up, wide_down = w_up.shape[0], w_down.shape[1]
    groups = lines.gather(pack(w_up, w_down))
    ups = [[piece[:deep_up] for piece in group] for group in groups]
    downs = [[unpack(piece[deep_up:], wide_down) for piece in group] for group in groups]
    order = lines.order()

    parts = []
    for h in range(heads):
        at_k, at_v = slice(h * depth, (h + 1) * depth), slice(h * width, (h + 1) * width)
        memory = one_head(
            queries[:, at_k],
            keys[:, at_k],
            values[:, at_v],
            input_gates[:, h],
            forget_gates[:, h],
            doc_pos,
            reach,
        )
        normed = memory * lax.rsqrt(jnp.mean(memory * memory, axis=-1, keepdims=True) + eps)
        gate = jax.nn.sigmoid(out_gate[:, at_v].astype(f32))
        parts.append((normed * head_gain[at_v] * gate).astype(bf16))
    readout = parts[0] if heads == 1 else jnp.concatenate(parts, axis=1)

    projected = dot(readout, w_out).astype(bf16).reshape(tps.far, tps.core, rows, -1)
    me = lax.axis_index("tp")
    x, c = me // tps.core, me % tps.core

    def for_core(core):
        picked = lax.dynamic_index_in_dim(projected, core, 1, False)
        return jnp.stack(
            [
                lax.dynamic_index_in_dim(picked, (x + tps.far - r) % tps.far, 0, False)
                for r in range(tps.far)
            ]
        )

    summed = tps.reduce(for_core(c), for_core(1 - c) if tps.core == 2 else None)
    mixed = resid.astype(f32) + summed
    factor = lax.rsqrt(jnp.mean(mixed * mixed, axis=-1, keepdims=True) + eps)
    scaled = (mixed * factor * norm_gain).astype(bf16)

    blocks = order.shape[0]
    deep = scaled.shape[1] // blocks
    turned = jnp.concatenate(
        [lax.dynamic_slice_in_dim(scaled, order[i] * deep, deep, 1) for i in range(blocks)], axis=1
    )
    up_full = jnp.concatenate([piece for group in ups for piece in group], axis=0)
    product = dot(tps.gather(turned), up_full)
    hidden = jnp.square(jax.nn.relu(product)).astype(bf16)

    bundle = max(1, len(downs) // 4)
    outs = []
    for at in range(0, len(downs), bundle):
        pieces = [piece for group in downs[at : at + bundle] for piece in group]
        part = dot(hidden, jnp.concatenate(pieces, axis=1)).astype(bf16)
        part = part.reshape(tps.core, tps.far, rows, -1)
        outs.append(tps.reduce(part[0], part[1] if tps.core == 2 else None))
    summed = jnp.concatenate(outs, axis=1)
    back = jnp.concatenate(
        [lax.dynamic_slice_in_dim(summed, lines.piece(i) * deep, deep, 1) for i in range(blocks)],
        axis=1,
    )
    return (mixed + back).astype(bf16)


class Spot:
    def __init__(self, n_sp, n_tp):
        self.n_sp, self.n_tp = n_sp, n_tp
        self.line = n_sp // 2
        self.sp = lax.axis_index("sp")
        self.tp = lax.axis_index("tp")
        self.z, self.y = self.sp // 2, self.sp % 2
        self.x, self.c = self.tp // 2, self.tp % 2
        self.zp = self.z % 2
        self.base = self.z - self.zp

    def at(self, z=None, y=None, x=None, c=None):
        z = self.z if z is None else z
        y = self.y if y is None else y
        x = self.x if x is None else x
        c = self.c if c is None else c
        return (z * 2 + y, x * 2 + c)


class Wire:
    def __init__(self, send_sems, recv_sems):
        self.send_sems, self.recv_sems = send_sems, recv_sems
        self.count = 0

    def slot(self):
        self.count += 1
        return self.count - 1

    def copy(self, src, dst, number, where, arrival=None):
        return pltpu.make_async_remote_copy(
            src_ref=src,
            dst_ref=dst,
            send_sem=self.send_sems.at[number],
            recv_sem=self.recv_sems.at[number if arrival is None else arrival],
            device_id=where,
            device_id_type=MESH,
        )


def layer_kernel(
    n_sp,
    n_tp,
    q_hbm,
    k_hbm,
    v_hbm,
    og_hbm,
    ig_ref,
    fg_ref,
    doc_ref,
    hg_ref,
    wo_hbm,
    res_hbm,
    ng_ref,
    wup_hbm,
    wdn_hbm,
    out_ref,
    q_s,
    k_s,
    v_s,
    og_s,
    wo_s,
    res_s,
    up_s,
    dn_s,
    rows_s,
    cols_s,
    num_s,
    stat_s,
    own_s,
    own_info_s,
    got_s,
    got_info_s,
    mid_s,
    mid_info_s,
    fin_s,
    read_s,
    heads_s,
    mixed_s,
    nrm_s,
    hid_s,
    part_s,
    r1_s,
    r2_out_s,
    r2_keep_s,
    r2_in_s,
    r3_out_s,
    r3_in_s,
    local_sem,
    send_sem,
    recv_sem,
):
    me = Spot(n_sp, n_tp)
    wire = Wire(send_sem, recv_sem)
    line = me.line
    length, depth = q_s.shape
    width = v_s.shape[1]
    rows = res_s.shape[0]
    deep = wup_hbm.shape[0]
    hidden = up_s.shape[2]
    wide = wdn_hbm.shape[1]
    scale = depth ** (-0.5)
    waits = []

    def start(copy, cond=None):
        if cond is None:
            copy.start()
            waits.append((copy, None))
        else:
            pl.when(cond)(copy.start)
            waits.append((copy, cond))

    def drain(copy):
        copy.wait_send()
        waits[:] = [item for item in waits if item[0] is not copy]

    def load(src, dst, number):
        copy = pltpu.make_async_copy(src, dst, local_sem.at[number])
        copy.start()
        return copy

    up_z = [[wire.slot() for _ in range(line)][0] for _ in range(2)]
    dn_z = [[wire.slot() for _ in range(line)][0] for _ in range(2)]
    up_y = [[wire.slot() for _ in range(line)][0] for _ in range(2)]
    dn_y = [[wire.slot() for _ in range(line)][0] for _ in range(2)]
    ends_line = (me.z == 0) | (me.z == line - 1)
    inner_line = jnp.logical_not(ends_line)

    planes = [me.z, me.base + 1 - me.zp]
    for i in range(2, line, 2):
        pair = lax.rem(me.base + i, line)
        planes += [pair + me.zp, pair + 1 - me.zp]
    up_part = [pl.ds(h * (deep // 2), deep // 2) for h in range(2)]
    dn_part = [pl.ds(h * (hidden // 2), hidden // 2) for h in range(2)]

    def up_piece(z, h):
        lanes = pl.ds(pl.multiple_of((z % 2) * hidden, hidden), hidden)
        return wup_hbm.at[up_part[h], lanes]

    def dn_piece(z, h):
        at = (z % 2) * hidden + h * (hidden // 2)
        return wdn_hbm.at[pl.ds(pl.multiple_of(at, hidden // 2), hidden // 2), :]

    def send_up(z, h, cond=None):
        dst = up_s.at[me.sp, up_part[h]]
        start(wire.copy(up_piece(z, h), dst, up_z[h] + z, me.at(z=z), up_z[h] + me.z), cond)

    def send_dn(z, h, cond=None):
        dst = dn_s.at[me.sp, dn_part[h]]
        copy = wire.copy(dn_piece(z, h), dst, dn_z[h] + z, me.at(z=z), dn_z[h] + me.z)
        start(copy, cond)
        return copy

    beside = me.at(y=1 - me.y)

    def over_up(z, h, own=False):
        ref = up_s.at[z * 2 + me.y, up_part[h]]
        return wire.copy(up_piece(z, h) if own else ref, ref, up_y[h] + z, beside)

    def over_dn(z, h, own=False):
        ref = dn_s.at[z * 2 + me.y, dn_part[h]]
        return wire.copy(dn_piece(z, h) if own else ref, ref, dn_y[h] + z, beside)

    def relay_up(z, h):
        ref = up_s.at[z * 2 + me.y, up_part[h]]
        wire.copy(ref, ref, up_z[h] + z, me.at(z=z)).wait_recv()
        start(over_up(z, h))

    def crossed_up(z, h):
        ref = up_s.at[z * 2 + 1 - me.y, up_part[h]]
        wire.copy(ref, ref, up_y[h] + z, beside).wait_recv()

    def crossed_dn(z, h):
        ref = dn_s.at[z * 2 + 1 - me.y, dn_part[h]]
        wire.copy(ref, ref, dn_y[h] + z, beside).wait_recv()

    k_in = load(k_hbm, k_s, 0)
    v_in = load(v_hbm, v_s, 1)
    q_in = load(q_hbm, q_s, 2)
    og_in = load(og_hbm, og_s, 3)
    wo_in = load(wo_hbm, wo_s.at[me.tp], 4)
    res_in = load(res_hbm, res_s, 5)
    own_in = []
    for h in range(2):
        own_in.append(load(up_piece(me.z, h), up_s.at[me.sp, up_part[h]], 6 + h))
    dn_in = [load(dn_piece(me.z, h), dn_s.at[me.sp, dn_part[h]], 8 + h) for h in range(2)]

    barrier = pltpu.get_barrier_semaphore()
    met = [me.at(z=z) for z in planes[1:]]
    met += [beside, me.at(c=1 - me.c), me.at(x=1 - me.x), me.at(x=1 - me.x, c=1 - me.c)]
    met += [(lax.rem(me.sp + i, n_sp), me.tp) for i in (1, n_sp - 1)]
    for where in met:
        pl.semaphore_signal(barrier, inc=1, device_id=where, device_id_type=MESH)
    pl.semaphore_wait(barrier, len(met))
    send_up(planes[2], 0)
    send_up(planes[1], 0)
    start(over_up(me.z, 0, True))
    wo_no = [wire.slot() for _ in range(3)]
    core = me.at(c=1 - me.c)
    over = me.at(x=1 - me.x)
    above = me.at(z=me.base + 1 - me.zp)
    far_x, far_c = 1 - me.x, 1 - me.c

    def heads_row(number, where, owner_tp, src=None):
        ref = wo_s.at[owner_tp]
        return wire.copy(ref if src is None else src, ref, number, where)

    start(heads_row(wo_no[0], over, me.tp, wo_hbm))
    start(heads_row(wo_no[1], core, me.tp, wo_hbm))
    lane = lax.broadcasted_iota(jnp.int32, (8, length), 1)
    sub = lax.broadcasted_iota(jnp.int32, (8, length), 0)
    pre = jnp.concatenate([fg_ref[0], fg_ref[1]], axis=0)
    logf = jnp.minimum(pre, 0.0) - jnp.log1p(jnp.exp(-jnp.abs(pre)))
    cum_f = jnp.broadcast_to(logf[0:1], (8, length))
    cum_b = jnp.broadcast_to(logf[1:2], (8, length))
    step = 1
    while step < length:
        cum_f = cum_f + jnp.where(lane >= step, pltpu.roll(cum_f, step, 1), 0.0)
        cum_b = cum_b + jnp.where(lane < length - step, pltpu.roll(cum_b, length - step, 1), 0.0)
        step *= 2
    gate = jnp.concatenate([ig_ref[0], ig_ref[1]], axis=0)
    rel_f = jnp.broadcast_to(gate[0:1], (8, length)) - cum_f
    rel_b = jnp.broadcast_to(gate[1:2], (8, length)) - cum_b
    doc = jnp.broadcast_to(doc_ref[...].reshape(1, length).astype(f32), (8, length))
    total_f, total_b = cum_f[:, length - 1 :], cum_b[:, 0:1]
    first, last = doc[:, 0:1], doc[:, length - 1 :]
    exp_f = jnp.where(doc == last, total_f + rel_f, far_low)
    exp_b = jnp.where(doc == first, total_b + rel_b, far_low)
    peak_f = jnp.max(exp_f, axis=1, keepdims=True)
    peak_b = jnp.max(exp_b, axis=1, keepdims=True)
    keep_f, keep_b = jnp.exp(exp_f - peak_f), jnp.exp(exp_b - peak_b)
    rows_s[...] = jnp.where(sub == 0, rel_f, jnp.where(sub == 1, rel_b, doc))
    table = jnp.where(sub == 0, cum_f, cum_b)
    table = jnp.where(sub == 2, doc, table)
    table = jnp.where(sub == 3, keep_f, table)
    table = jnp.where(sub == 4, keep_b, table)
    cols_s[...] = table.T

    k_in.wait()
    v_in.wait()
    wide_keys = k_s[...].astype(f32)

    def own(d, column, peak, total, doc_out):
        weighted = (wide_keys * cols_s[:, column : column + 1]).astype(bf16)
        norm = jnp.sum(weighted.astype(f32), axis=0, keepdims=True)
        own_s[d] = lax.dot_general(
            weighted, v_s[...], (((0,), (0,)), ((), ())), preferred_element_type=f32
        ).astype(bf16)
        at = lax.broadcasted_iota(jnp.int32, (8, depth), 0)
        info = jnp.where(at == 0, jnp.broadcast_to(norm, (8, depth)), peak)
        info = jnp.where(at == 2, total, info)
        own_info_s[d] = jnp.where(at == 3, doc_out, info)

    own(0, 3, peak_f, total_f, last)
    own(1, 4, peak_b, total_b, first)

    def reach_of(d, far):
        sign = 1 if d == 0 else -1
        to, frm = me.sp + sign * far, me.sp - sign * far
        can_send = (to < n_sp) if d == 0 else (to >= 0)
        can_recv = (frm >= 0) if d == 0 else (frm < n_sp)
        return to, can_send, can_recv

    state_no = [[(wire.slot(), wire.slot()) for _ in range(2)] for _ in range(3)]

    def state_copies(r, d, far, src, info):
        to, can_send, can_recv = reach_of(d, far)
        to = jnp.clip(to, 0, n_sp - 1)
        a, b = state_no[r][d]
        return (
            wire.copy(src.at[d], got_s.at[r, d], a, (to, me.tp)),
            wire.copy(info.at[d], got_info_s.at[r, d], b, (to, me.tp)),
            can_send,
            can_recv,
        )

    def state_send(r, d, far, src, info):
        mem, note, can_send, can_recv = state_copies(r, d, far, src, info)
        start(note, can_send)
        start(mem, can_send)

        @pl.when(jnp.logical_not(can_recv))
        def _():
            got_s[r, d] = jnp.zeros(got_s.shape[2:], bf16)
            got_info_s[r, d] = jnp.full(got_info_s.shape[2:], -1.0, f32)

    def state_recv(r, d, far, src, info):
        mem, note, _, can_recv = state_copies(r, d, far, src, info)

        @pl.when(can_recv)
        def _():
            note.wait_recv()
            mem.wait_recv()

    for far in (1, 2):
        for d in (0, 1):
            state_send(far - 1, d, far, own_s, own_info_s)
    send_up(planes[2], 1)
    send_up(planes[1], 1)
    start(over_up(me.z, 1, True))

    q_in.wait()

    def inside(j, carry):
        r0 = pl.multiple_of(j * rows, rows)
        score = (
            lax.dot_general(
                q_s[pl.ds(r0, rows), :],
                k_s[...],
                (((1,), (1,)), ((), ())),
                preferred_element_type=f32,
            )
            * scale
        )
        at_row = lax.broadcasted_iota(jnp.int32, (rows, length), 0) + r0
        at_col = lax.broadcasted_iota(jnp.int32, (rows, length), 1)
        cols = cols_s[pl.ds(r0, rows), :]
        same = cols[:, 2:3] == rows_s[2:3, :]
        for d in (0, 1):
            order = (at_row >= at_col) if d == 0 else (at_row <= at_col)
            exponent = jnp.where(
                same & order, cols[:, d : d + 1] + rows_s[d : d + 1, :], far_low
            )
            top = jnp.max(exponent, axis=1, keepdims=True)
            weights = score * jnp.exp(exponent - top)
            stat_s[2 * d, pl.ds(r0, rows), :] = top
            stat_s[2 * d + 1, pl.ds(r0, rows), :] = jnp.sum(weights, axis=1, keepdims=True)
            num_s[d, pl.ds(r0, rows), :] = jnp.dot(
                weights.astype(bf16), v_s[...], preferred_element_type=f32
            )
        return carry

    lax.fori_loop(0, length // rows, inside, 0)

    def info_row(r, d, i):
        return got_info_s[r, d, i : i + 1, :]

    near = []
    for d in (0, 1):
        here = (first if d == 0 else last)[0:1]
        state_recv(0, d, 1, own_s, own_info_s)
        state_recv(1, d, 2, own_s, own_info_s)
        link1 = info_row(0, d, 3) == here
        link2 = info_row(1, d, 3) == here
        level1 = jnp.where(link1, info_row(0, d, 1), far_low)
        level2 = jnp.where(link2, info_row(1, d, 1) + info_row(0, d, 2), far_low)
        top = jnp.maximum(level1, level2)
        share1 = jnp.where(link1, jnp.exp(level1 - top), 0.0)
        share2 = jnp.where(link2, jnp.exp(level2 - top), 0.0)
        norm = share1 * info_row(0, d, 0) + share2 * info_row(1, d, 0)
        mid_s[d] = (
            share1[:, 0:1] * got_s[0, d].astype(f32) + share2[:, 0:1] * got_s[1, d].astype(f32)
        ).astype(bf16)
        at = lax.broadcasted_iota(jnp.int32, (8, depth), 0)
        mid_info_s[d] = jnp.where(at == 0, norm, jnp.where(at == 1, top, here))
        state_send(2, d, 2, mid_s, mid_info_s)
        near.append((here, top, norm))

    relay_up(planes[2], 0)
    relay_up(planes[1], 0)

    ends = []
    for d in (0, 1):
        here, top, norm = near[d]
        state_recv(2, d, 2, mid_s, mid_info_s)
        link = info_row(2, d, 3) == here
        level = jnp.where(
            link, info_row(2, d, 1) + info_row(1, d, 2) + info_row(0, d, 2), far_low
        )
        peak = jnp.maximum(top, level)
        link1 = info_row(0, d, 3) == here
        share = jnp.where(link1, jnp.exp(top - peak), 0.0)
        share_far = jnp.where(link, jnp.exp(level - peak), 0.0)
        fin_s[d] = (
            share[:, 0:1] * mid_s[d].astype(f32) + share_far[:, 0:1] * got_s[2, d].astype(f32)
        ).astype(bf16)
        meets = jnp.where(link1, here, -2.0)
        ends.append((meets[:, 0:1], peak, share * norm + share_far * info_row(2, d, 0)))

    for h in range(2):
        for i in range(3, line):
            send_up(planes[i], h)
    send_dn(planes[2], 0)
    og_in.wait()

    def project(j):
        r0 = pl.multiple_of(j * rows, rows)
        queries = q_s[pl.ds(r0, rows), :]
        wide_q = queries.astype(f32)
        cols = cols_s[pl.ds(r0, rows), :]
        memory = None
        for d in (0, 1):
            meets, level, norm = ends[d]
            usable = cols[:, 2:3] == meets
            carried = jnp.where(usable, cols[:, d : d + 1] + level[:, 0:1], far_low)
            top = stat_s[2 * d, pl.ds(r0, rows), :]
            peak = jnp.maximum(carried, top)
            local = jnp.exp(top - peak)
            inter = jnp.where(usable, jnp.exp(carried - peak), 0.0) * scale
            den = local * stat_s[2 * d + 1, pl.ds(r0, rows), :] + inter * jnp.sum(
                wide_q * norm, axis=1, keepdims=True
            )
            under = 1.0 / jnp.maximum(jnp.abs(den), 1.0)
            term = (local * under) * num_s[d, pl.ds(r0, rows), :] + (inter * under) * jnp.dot(
                queries, fin_s[d], preferred_element_type=f32
            )
            memory = term if memory is None else memory + term
        normed = memory * lax.rsqrt(jnp.mean(memory * memory, axis=1, keepdims=True) + eps)
        open_gate = jax.nn.sigmoid(og_s[pl.ds(r0, rows), :].astype(f32))
        read_s[j] = (normed * hg_ref[...].reshape(1, width) * open_gate).astype(bf16)

    ro_no = [wire.slot() for _ in range(3)]
    peers = [(far_x, far_c), (far_x, me.c), (me.x, far_c)]

    def exchange(i):
        x, c = peers[i]
        return wire.copy(read_s.at[x * 2 + c], heads_s.at[me.tp], ro_no[i], me.at(x=x, c=c))

    for i in range(3):
        project(peers[i][0] * 2 + peers[i][1])
        start(exchange(i))
    project(me.tp)
    relay_up(planes[1], 1)
    relay_up(planes[2], 1)
    who_wo = far_x * 2 + me.c
    heads_row(wo_no[0], over, who_wo).wait_recv()
    start(heads_row(wo_no[2], core, who_wo))
    res_in.wait()
    wo_in.wait()

    def head_part(rows_ref, owner_tp):
        part = jnp.dot(rows_ref[...], wo_s[owner_tp], preferred_element_type=f32)
        return part.astype(bf16).astype(f32)

    mixed_s[...] = res_s[...].astype(f32) + head_part(read_s.at[me.tp], me.tp)
    for i in (2, 1, 0):
        x, c = peers[i]
        frm = x * 2 + c
        if i == 2:
            heads_row(wo_no[1], core, frm).wait_recv()
        if i == 0:
            heads_row(wo_no[2], core, frm).wait_recv()
        wire.copy(read_s.at[me.tp], heads_s.at[frm], ro_no[i], me.at(x=x, c=c)).wait_recv()
        mixed_s[...] += head_part(heads_s.at[frm], frm)
    mixed = mixed_s[...]
    factor = lax.rsqrt(jnp.mean(mixed * mixed, axis=1, keepdims=True) + eps)
    mine = me.zp * n_tp + me.tp
    nrm_s[mine] = (mixed * factor * ng_ref[...].reshape(1, nrm_s.shape[2])).astype(bf16)

    inner = jnp.where(me.base == 0, 1, me.base)
    others = [
        jnp.where(me.base == 0, 2 + i, lax.rem(me.base + line - 1 - i, line))
        for i in range(line - 2)
    ]
    course = [others[0], inner] + others[1:] + [2 * me.base + 1 - inner]
    order = []
    for z in course:
        order += [(z, me.y), (z, 1 - me.y)]

    def relay_dn(z, h, cond=None):
        ref = dn_s.at[z * 2 + me.y, dn_part[h]]
        got = wire.copy(ref, ref, dn_z[h] + z, me.at(z=z))
        if cond is None:
            got.wait_recv()
        else:
            pl.when(cond)(got.wait_recv)
        start(over_dn(z, h), cond)

    def owner(zp, x, c):
        return zp * n_tp + x * 2 + c

    far_z = 1 - me.zp
    n_core = [wire.slot() for _ in range(4)]
    n_x, n_z, n_xh = wire.slot(), wire.slot(), wire.slot()

    def pass_on(number, where, who, part=None):
        ref = nrm_s.at[who] if part is None else nrm_s.at[who, part]
        return wire.copy(ref, ref, number, where)

    start(pass_on(n_x, over, mine))
    start(pass_on(n_z, above, mine))
    start(pass_on(n_core[0], core, mine))
    send_dn(planes[2], 1)
    for h in range(2):
        for i in range(3, line):
            send_dn(planes[i], h, inner_line)
    for h in range(2):
        start(over_dn(me.z, h, True))

    def raise_rows(zp, x):
        group = zp * 2 + x

        def chunk(n, carry):
            c0 = pl.multiple_of(n * 256, 256)
            left = nrm_s[pl.ds(group * 2, 2), :, :].reshape(2 * rows, nrm_s.shape[2])
            right = up_s[:, :, pl.ds(c0, 256)].reshape(n_sp * deep, 256)
            pre = jnp.maximum(jnp.dot(left, right, preferred_element_type=f32), 0.0)
            hid_s[group, :, pl.ds(c0, 256)] = (pre * pre).astype(bf16)
            return carry

        lax.fori_loop(0, hidden // 256, chunk, 0)

    who = owner(me.zp, far_x, me.c)
    pass_on(n_x, over, who).wait_recv()
    start(pass_on(n_core[1], core, who))
    near_dn = [send_dn(planes[1], h) for h in range(2)]
    for h in range(2):
        for i in range(3, line):
            relay_up(planes[i], h)
    relay_dn(planes[2], 0)
    who = owner(far_z, me.x, me.c)
    pass_on(n_z, above, who).wait_recv()
    start(pass_on(n_xh, over, who))
    start(pass_on(n_core[2], core, who))
    for copy in own_in:
        copy.wait()
    for z in planes:
        for h in range(2):
            crossed_up(z, h)
    pass_on(n_core[0], core, owner(me.zp, me.x, far_c)).wait_recv()
    raise_rows(me.zp, me.x)
    pass_on(n_core[1], core, owner(me.zp, far_x, far_c)).wait_recv()
    raise_rows(me.zp, far_x)
    pass_on(n_core[2], core, owner(far_z, me.x, far_c)).wait_recv()
    raise_rows(far_z, me.x)
    relay_dn(planes[2], 1)
    for h in range(2):
        for i in range(3, line):
            relay_dn(planes[i], h, inner_line)
    who = owner(far_z, far_x, me.c)
    pass_on(n_xh, over, who).wait_recv()
    start(pass_on(n_core[3], core, who))
    pass_on(n_core[3], core, owner(far_z, far_x, far_c)).wait_recv()
    for copy in near_dn:
        drain(copy)
    for h in range(2):
        for i in range(3, line):
            send_dn(planes[i], h, ends_line)
    raise_rows(far_z, far_x)
    for copy in dn_in:
        copy.wait()

    blocks = n_sp
    r1_no = [wire.slot() for _ in range(blocks)]
    r2_no = [wire.slot() for _ in range(blocks)]
    r3_no = [wire.slot() for _ in range(blocks)]
    groups = 4

    def lower(k):
        z, y = order[k]
        if k == 0:
            relay_dn(planes[1], 0, ends_line)
        if k == 1:
            relay_dn(planes[1], 1, ends_line)
        if k == 3:
            for h in range(2):
                for i in range(3, line):
                    relay_dn(planes[i], h, ends_line)
        if k == 5:
            for h in range(2):
                relay_dn(planes[1], h, inner_line)
        if k % 2 == 1:
            for h in range(2):
                crossed_dn(z, h)
        slot = z * 2 + y

        def one(g, carry):
            value = jnp.dot(hid_s[g], dn_s[slot], preferred_element_type=f32).astype(bf16)
            part_s[k, 0, g] = value[:rows]
            part_s[k, 1, g] = value[rows:]
            return carry

        lax.fori_loop(0, groups, one, 0)
        start(wire.copy(part_s.at[k, far_c], r1_s.at[k], r1_no[k], core))

    def sum1(k):
        wire.copy(part_s.at[k, far_c], r1_s.at[k], r1_no[k], core).wait_recv()

        def both(g):
            return part_s[k, me.c, g].astype(f32) + r1_s[k, g].astype(f32)

        for i in range(2):
            away = i * 2 + far_x
            r2_out_s[k, i] = both(away).astype(bf16)
        start(wire.copy(r2_out_s.at[k], r2_in_s.at[k], r2_no[k], over))
        for i in range(2):
            here = i * 2 + me.x
            r2_keep_s[k, i] = both(here)

    def sum2(k):
        wire.copy(
            r2_out_s.at[k], r2_in_s.at[k], r2_no[k], over
        ).wait_recv()
        far = far_z
        r3_out_s[k] = (r2_keep_s[k, far] + r2_in_s[k, far].astype(f32)).astype(bf16)
        start(wire.copy(r3_out_s.at[k], r3_in_s.at[k], r3_no[k], above))

    def sum3(k):
        wire.copy(
            r3_out_s.at[k], r3_in_s.at[k], r3_no[k], above
        ).wait_recv()
        z, y = order[k]
        c0 = pl.multiple_of((z * 2 + y) * wide, wide)
        at = me.zp
        total = r2_keep_s[k, at] + r2_in_s[k, at].astype(f32) + r3_in_s[k].astype(f32)
        total = mixed_s[:, pl.ds(c0, wide)] + total
        out_ref[:, pl.ds(c0, wide)] = total.astype(bf16)

    for k in range(blocks + 4):
        if k < blocks:
            lower(k)
        if 0 <= k - 1 < blocks:
            sum1(k - 1)
        if 0 <= k - 2 < blocks:
            sum2(k - 2)
        if 0 <= k - 4 < blocks:
            sum3(k - 4)

    for copy, cond in waits:
        if cond is None:
            copy.wait_send()
        else:
            pl.when(cond)(copy.wait_send)


def fused(n_sp, n_tp, *args):
    (
        queries,
        keys,
        values,
        out_gate,
        input_gates,
        forget_gates,
        doc_ids,
        head_gain,
        w_out,
        resid,
        norm_gain,
        w_up,
        w_down,
    ) = args
    length, depth = queries.shape
    width = values.shape[1]
    rows, model = resid.shape
    deep, wide = w_up.shape[0], w_down.shape[1]
    hidden = w_up.shape[1] // 2
    line = n_sp // 2
    blocks = n_sp
    numbers = 8 * line + 27 + 3 * blocks
    vmem = pltpu.VMEM
    scratch = [
        vmem((length, depth), bf16),
        vmem((length, depth), bf16),
        vmem((length, width), bf16),
        vmem((length, width), bf16),
        vmem((n_tp, width, model), bf16),
        vmem((rows, model), bf16),
        vmem((n_sp, deep, hidden), bf16),
        vmem((n_sp, hidden, wide), bf16),
        vmem((8, length), f32),
        vmem((length, 8), f32),
        vmem((2, length, width), f32),
        vmem((4, length, 1), f32),
        vmem((2, depth, width), bf16),
        vmem((2, 8, depth), f32),
        vmem((3, 2, depth, width), bf16),
        vmem((3, 2, 8, depth), f32),
        vmem((2, depth, width), bf16),
        vmem((2, 8, depth), f32),
        vmem((2, depth, width), bf16),
        vmem((n_tp, rows, width), bf16),
        vmem((n_tp, rows, width), bf16),
        vmem((rows, model), f32),
        vmem((2 * n_tp, rows, model), bf16),
        vmem((4, 2 * rows, hidden), bf16),
        vmem((blocks, 2, 4, rows, wide), bf16),
        vmem((blocks, 4, rows, wide), bf16),
        vmem((blocks, 2, rows, wide), bf16),
        vmem((blocks, 2, rows, wide), f32),
        vmem((blocks, 2, rows, wide), bf16),
        vmem((blocks, rows, wide), bf16),
        vmem((blocks, rows, wide), bf16),
        pltpu.SemaphoreType.DMA((10,)),
        pltpu.SemaphoreType.DMA((numbers,)),
        pltpu.SemaphoreType.DMA((numbers,)),
    ]
    anywhere = pl.BlockSpec(memory_space=pl.ANY)
    inside = pl.BlockSpec(memory_space=pltpu.VMEM)
    return pl.pallas_call(
        functools.partial(layer_kernel, n_sp, n_tp),
        out_shape=jax.ShapeDtypeStruct((rows, model), bf16),
        in_specs=[anywhere] * 4 + [inside] * 4 + [anywhere] * 2 + [inside] + [anywhere] * 2,
        out_specs=inside,
        scratch_shapes=scratch,
        compiler_params=pltpu.CompilerParams(
            collective_id=0, has_side_effects=True, vmem_limit_bytes=66_000_000
        ),
        name="layer",
    )(
        queries,
        keys,
        values,
        out_gate,
        input_gates,
        forget_gates,
        doc_ids,
        head_gain,
        w_out,
        resid,
        norm_gain,
        w_up,
        w_down,
    )


def fits(mesh, args):
    n_sp, n_tp = mesh.shape["sp"], mesh.shape["tp"]
    queries, input_gates, w_up, w_down = args[0], args[4], args[11], args[12]
    length = queries.shape[0] // n_sp
    return (
        n_tp == 4
        and n_sp % 4 == 0
        and input_gates.shape[1] == n_tp
        and -(-longest_doc // length) <= 4
        and length % (n_tp * 32) == 0
        and w_down.shape[1] % (n_sp * 128) == 0
        and w_up.shape[0] % (n_sp * 16) == 0
        and w_up.shape[1] % (n_tp * 512) == 0
    )


def solution(mesh):
    in_specs = (
        P("sp", "tp"),
        P("sp", "tp"),
        P("sp", "tp"),
        P("sp", "tp"),
        P(None, "tp", "sp"),
        P(None, "tp", "sp"),
        P("sp"),
        P("tp"),
        P("tp", None),
        P(("sp", "tp"), None),
        P(),
        P("sp", "tp"),
        P("tp", "sp"),
    )
    out_specs = P(("sp", "tp"), None)

    def step(*args):
        whole = fits(mesh, args)
        body = functools.partial(fused, mesh.shape["sp"], mesh.shape["tp"]) if whole else shards
        return jax.shard_map(
            body, mesh=mesh, in_specs=in_specs, out_specs=out_specs, check_vma=False
        )(*args)

    return step
```

```python
import functools

import jax
import jax.numpy as jnp
from jax import lax
from jax.experimental import pallas as pl
from jax.experimental.pallas import tpu as pltpu
from jax.sharding import PartitionSpec as P


eps = 1e-06
far_low = -1e30
longest_doc = 3072


MESH = pl.DeviceIdType.MESH
bf16 = jnp.bfloat16
f32 = jnp.float32


def dot(a, b):
    return jnp.dot(a, b, preferred_element_type=f32)


class Lines:
    def __init__(self):
        count = lax.axis_size("sp")
        self.pair = 2 if count % 2 == 0 else 1
        self.line = count // self.pair

    def along(self, value, step):
        table = [
            (z * self.pair + y, (z + step) * self.pair + y)
            for z in range(self.line)
            for y in range(self.pair)
            if 0 <= z + step < self.line
        ]
        return lax.ppermute(value, "sp", table)

    def across(self, value, valid):
        table = [
            (z * self.pair + y, z * self.pair + 1 - y)
            for z in range(self.line)
            if valid(z)
            for y in range(self.pair)
        ]
        return lax.ppermute(value, "sp", table)

    def order(self):
        place = lax.axis_index("sp")
        z, y = place // self.pair, place % self.pair
        sources = []
        for k in range(self.line):
            row = (z + self.line - k) % self.line
            sources.append(row * self.pair + y)
            if self.pair == 2:
                sources.append(row * self.pair + 1 - y)
        return jnp.stack(sources)

    def piece(self, source):
        place = lax.axis_index("sp")
        z, y = place // self.pair, place % self.pair
        k = (z + self.line - source // self.pair) % self.line
        return k * self.pair + (y + source) % self.pair

    def gather(self, own):
        n = self.line
        up, down = {}, {}
        up_side, down_side = {}, {}
        two = self.pair == 2
        own_side = self.across(own, lambda z: True) if two else None
        prev_up = prev_down = own
        for k in range(1, n):
            prev_up = up[k] = self.along(prev_up, 1)
            prev_down = down[k] = self.along(prev_down, -1)
            if two:
                up_side[k] = self.across(prev_up, lambda z: z >= k)
                down_side[k] = self.across(prev_down, lambda z: z + k < n)
        groups = [[own] + ([own_side] if two else [])]
        z = lax.axis_index("sp") // self.pair
        for k in range(1, n):
            below = z >= k
            group = [jnp.where(below, up[k], down[n - k])]
            if two:
                group.append(jnp.where(below, up_side[k], down_side[n - k]))
            groups.append(group)
        return groups


class Heads:
    def __init__(self):
        count = lax.axis_size("tp")
        self.core = 2 if count % 2 == 0 else 1
        self.far = count // self.core

    def swap(self, value):
        count = lax.axis_size("tp")
        return lax.ppermute(value, "tp", [(i, i ^ 1) for i in range(count)])

    def shift(self, value, step):
        table = [
            (x * self.core + c, ((x + step) % self.far) * self.core + c)
            for x in range(self.far)
            for c in range(self.core)
        ]
        return lax.ppermute(value, "tp", table)

    def gather(self, own):
        mine = [own] + [self.shift(own, r) for r in range(1, self.far)]
        if self.core == 1:
            return jnp.concatenate(mine)
        return jnp.concatenate(mine + [self.swap(block) for block in mine])

    def reduce(self, near, away):
        total = near.astype(f32)
        if away is not None:
            total = total + self.swap(away).astype(f32)
        out = total[0]
        for r in range(1, self.far):
            out = out + self.shift(total[r].astype(bf16), -r).astype(f32)
        return out


def local_part(scores, values, exponent, keep):
    top = jnp.max(jnp.where(keep, exponent, far_low), axis=1)
    weights = jnp.where(keep, scores * jnp.exp(exponent - top[:, None]), 0.0)
    return top, dot(weights.astype(bf16), values), jnp.sum(weights, axis=1)


def summary(keys, exponent):
    peak = jnp.max(exponent)
    weighted = (keys * jnp.exp(exponent - peak)[:, None]).astype(bf16)
    return weighted, jnp.sum(weighted.astype(f32), axis=0), peak


def split_row(row, width):
    terms, rest = [], row
    for _ in range(3):
        term = lax.reduce_precision(rest, 8, 7)
        rest = rest - term
        terms.append(term.astype(bf16))
    lines = -(-row.shape[0] // width)
    table = jnp.stack([jnp.pad(t, (0, lines * width - t.shape[0])) for t in terms])
    table = table.reshape(3 * lines, width)
    return jnp.pad(table, ((0, -(3 * lines) % 16), (0, 0)))


def join_row(table, size):
    lines = -(-size // table.shape[1])
    terms = table[: 3 * lines].astype(f32).reshape(3, -1)
    return (terms[0] + terms[1] + terms[2])[:size]


def incoming(memory, row, doc_here, sign, reach):
    count = lax.axis_size("sp")
    place = lax.axis_index("sp")
    depth, width = memory.shape
    sent = jnp.concatenate([memory, split_row(row, width)])
    arrived = []
    for d in range(1, min(reach, count - 1) + 1):
        table = [(i, i + sign * d) for i in range(count) if 0 <= i + sign * d < count]
        got = lax.ppermute(sent, "sp", table)
        arrived.append((join_row(got[depth:], row.shape[0]), got[:depth]))
    passed = jnp.zeros((), f32)
    levels, linked = [], []
    for d, (got, _) in enumerate(arrived, 1):
        there = (place >= d) if sign > 0 else (place + d < count)
        joined = there & (got[depth + 2] == doc_here)
        levels.append(jnp.where(joined, got[depth] + passed, far_low))
        linked.append(joined)
        passed = passed + got[depth + 1]
    top = jnp.max(jnp.stack(levels))
    state = jnp.zeros(memory.shape, f32)
    norm = jnp.zeros((depth,), f32)
    for level, joined, (got, mem) in zip(levels, linked, arrived):
        share = jnp.where(joined, jnp.exp(level - top), 0.0)
        state = state + share * mem.astype(f32)
        norm = norm + share * got[:depth]
    return state.astype(bf16), norm, top, linked[0]


def one_head(queries, keys, values, in_gates, forget_pre, doc_pos, reach):
    length, depth = queries.shape
    scale = depth ** (-0.5)
    place = jnp.arange(length)
    logf = jax.nn.log_sigmoid(forget_pre)
    before = place[:, None] >= place[None, :]
    after = place[:, None] <= place[None, :]
    cum_f = jnp.sum(jnp.where(before, logf[0][None, :], 0.0), axis=1)
    cum_b = jnp.sum(jnp.where(after, logf[1][None, :], 0.0), axis=1)
    total_f, total_b = cum_f[length - 1], cum_b[0]
    first, last = doc_pos[0], doc_pos[length - 1]
    weighted_f, norm_f, peak_f = summary(
        keys, jnp.where(doc_pos == last, total_f - cum_f + in_gates[0], far_low)
    )
    weighted_b, norm_b, peak_b = summary(
        keys, jnp.where(doc_pos == first, total_b - cum_b + in_gates[1], far_low)
    )

    def own_state(weighted):
        return lax.dot_general(
            weighted, values, (((0,), (0,)), ((), ())), preferred_element_type=f32
        ).astype(bf16)

    pad = jnp.zeros((125,), f32)
    row_f = jnp.concatenate([norm_f, jnp.stack([peak_f, total_f, last]), pad])
    row_b = jnp.concatenate([norm_b, jnp.stack([peak_b, total_b, first]), pad])
    state_f, norm_in_f, top_f, has_f = incoming(own_state(weighted_f), row_f, first, 1, reach)
    state_b, norm_in_b, top_b, has_b = incoming(own_state(weighted_b), row_b, last, -1, reach)

    scores = (
        lax.dot_general(queries, keys, (((1,), (1,)), ((), ())), preferred_element_type=f32) * scale
    )
    same = doc_pos[:, None] == doc_pos[None, :]
    wide = queries.astype(f32)

    def finish(cum, gate, keep, state, norm_in, top_in, usable):
        exponent = cum[:, None] - cum[None, :] + gate[None, :]
        top, numer, denom = local_part(scores, values, exponent, keep)
        carried = jnp.where(usable, cum + top_in, far_low)
        peak = jnp.maximum(carried, top)
        local = jnp.exp(top - peak)
        inter = jnp.where(usable, jnp.exp(carried - peak), 0.0) * scale
        denom = local * denom + inter * jnp.sum(wide * norm_in[None, :], axis=1)
        under = 1.0 / jnp.maximum(jnp.abs(denom), 1.0)
        return (local * under)[:, None] * numer + (inter * under)[:, None] * dot(queries, state)

    return finish(
        cum_f, in_gates[0], before & same, state_f, norm_in_f, top_f, has_f & (doc_pos == first)
    ) + finish(
        cum_b, in_gates[1], after & same, state_b, norm_in_b, top_b, has_b & (doc_pos == last)
    )


def pack(w_up, w_down):
    wide = w_down.shape[1]
    count = w_up.shape[1] // wide
    tiles = [w_down[i * wide : (i + 1) * wide] for i in range(count)]
    return jnp.concatenate([w_up, jnp.concatenate(tiles, axis=1)])


def unpack(table, wide):
    count = table.shape[1] // wide
    return jnp.concatenate([table[:, i * wide : (i + 1) * wide] for i in range(count)])


def shards(*args):
    return layer(*args)


def layer(
    queries,
    keys,
    values,
    out_gate,
    input_gates,
    forget_gates,
    doc_ids,
    head_gain,
    w_out,
    resid,
    norm_gain,
    w_up,
    w_down,
):
    length = queries.shape[0]
    heads = input_gates.shape[1]
    depth, width = queries.shape[1] // heads, values.shape[1] // heads
    lines, tps = Lines(), Heads()
    rows = resid.shape[0]
    doc_pos = doc_ids.astype(f32)
    reach = -(-longest_doc // length)
    deep_up, wide_down = w_up.shape[0], w_down.shape[1]
    groups = lines.gather(pack(w_up, w_down))
    ups = [[piece[:deep_up] for piece in group] for group in groups]
    downs = [[unpack(piece[deep_up:], wide_down) for piece in group] for group in groups]
    order = lines.order()

    parts = []
    for h in range(heads):
        at_k, at_v = slice(h * depth, (h + 1) * depth), slice(h * width, (h + 1) * width)
        memory = one_head(
            queries[:, at_k],
            keys[:, at_k],
            values[:, at_v],
            input_gates[:, h],
            forget_gates[:, h],
            doc_pos,
            reach,
        )
        normed = memory * lax.rsqrt(jnp.mean(memory * memory, axis=-1, keepdims=True) + eps)
        gate = jax.nn.sigmoid(out_gate[:, at_v].astype(f32))
        parts.append((normed * head_gain[at_v] * gate).astype(bf16))
    readout = parts[0] if heads == 1 else jnp.concatenate(parts, axis=1)

    projected = dot(readout, w_out).astype(bf16).reshape(tps.far, tps.core, rows, -1)
    me = lax.axis_index("tp")
    x, c = me // tps.core, me % tps.core

    def for_core(core):
        picked = lax.dynamic_index_in_dim(projected, core, 1, False)
        return jnp.stack(
            [
                lax.dynamic_index_in_dim(picked, (x + tps.far - r) % tps.far, 0, False)
                for r in range(tps.far)
            ]
        )

    summed = tps.reduce(for_core(c), for_core(1 - c) if tps.core == 2 else None)
    mixed = resid.astype(f32) + summed
    factor = lax.rsqrt(jnp.mean(mixed * mixed, axis=-1, keepdims=True) + eps)
    scaled = (mixed * factor * norm_gain).astype(bf16)

    blocks = order.shape[0]
    deep = scaled.shape[1] // blocks
    turned = jnp.concatenate(
        [lax.dynamic_slice_in_dim(scaled, order[i] * deep, deep, 1) for i in range(blocks)], axis=1
    )
    up_full = jnp.concatenate([piece for group in ups for piece in group], axis=0)
    product = dot(tps.gather(turned), up_full)
    hidden = jnp.square(jax.nn.relu(product)).astype(bf16)

    bundle = max(1, len(downs) // 4)
    outs = []
    for at in range(0, len(downs), bundle):
        pieces = [piece for group in downs[at : at + bundle] for piece in group]
        part = dot(hidden, jnp.concatenate(pieces, axis=1)).astype(bf16)
        part = part.reshape(tps.core, tps.far, rows, -1)
        outs.append(tps.reduce(part[0], part[1] if tps.core == 2 else None))
    summed = jnp.concatenate(outs, axis=1)
    back = jnp.concatenate(
        [lax.dynamic_slice_in_dim(summed, lines.piece(i) * deep, deep, 1) for i in range(blocks)],
        axis=1,
    )
    return (mixed + back).astype(bf16)


class Spot:
    def __init__(self, n_sp, n_tp):
        self.n_sp, self.n_tp = n_sp, n_tp
        self.line = n_sp // 2
        self.sp = lax.axis_index("sp")
        self.tp = lax.axis_index("tp")
        self.z, self.y = self.sp // 2, self.sp % 2
        self.x, self.c = self.tp // 2, self.tp % 2
        self.zp = self.z % 2
        self.base = self.z - self.zp

    def at(self, z=None, y=None, x=None, c=None):
        z = self.z if z is None else z
        y = self.y if y is None else y
        x = self.x if x is None else x
        c = self.c if c is None else c
        return (z * 2 + y, x * 2 + c)


class Wire:
    def __init__(self, send_sems, recv_sems):
        self.send_sems, self.recv_sems = send_sems, recv_sems
        self.count = 0

    def slot(self):
        self.count += 1
        return self.count - 1

    def copy(self, src, dst, number, where, arrival=None):
        return pltpu.make_async_remote_copy(
            src_ref=src,
            dst_ref=dst,
            send_sem=self.send_sems.at[number],
            recv_sem=self.recv_sems.at[number if arrival is None else arrival],
            device_id=where,
            device_id_type=MESH,
        )


def layer_kernel(
    n_sp,
    n_tp,
    q_hbm,
    k_hbm,
    v_hbm,
    og_hbm,
    ig_ref,
    fg_ref,
    doc_ref,
    hg_ref,
    wo_hbm,
    res_hbm,
    ng_ref,
    wup_hbm,
    wdn_hbm,
    out_ref,
    q_s,
    k_s,
    v_s,
    og_s,
    wo_s,
    res_s,
    up_s,
    dn_s,
    rows_s,
    cols_s,
    num_s,
    stat_s,
    own_s,
    own_info_s,
    got_s,
    got_info_s,
    mid_s,
    mid_info_s,
    fin_s,
    read_s,
    heads_s,
    mixed_s,
    nrm_s,
    hid_s,
    part_s,
    r1_s,
    r2_out_s,
    r2_keep_s,
    r2_in_s,
    r3_out_s,
    r3_in_s,
    local_sem,
    send_sem,
    recv_sem,
):
    me = Spot(n_sp, n_tp)
    wire = Wire(send_sem, recv_sem)
    line = me.line
    length, depth = q_s.shape
    width = v_s.shape[1]
    rows = res_s.shape[0]
    deep = wup_hbm.shape[0]
    hidden = up_s.shape[2]
    wide = wdn_hbm.shape[1]
    scale = depth ** (-0.5)
    waits = []

    def start(copy, cond=None):
        if cond is None:
            copy.start()
            waits.append((copy, None))
        else:
            pl.when(cond)(copy.start)
            waits.append((copy, cond))

    def drain(copy):
        copy.wait_send()
        waits[:] = [item for item in waits if item[0] is not copy]

    def load(src, dst, number):
        copy = pltpu.make_async_copy(src, dst, local_sem.at[number])
        copy.start()
        return copy

    up_z = [[wire.slot() for _ in range(line)][0] for _ in range(2)]
    dn_z = [[wire.slot() for _ in range(line)][0] for _ in range(2)]
    up_y = [[wire.slot() for _ in range(line)][0] for _ in range(2)]
    dn_y = [[wire.slot() for _ in range(line)][0] for _ in range(2)]
    ends_line = (me.z == 0) | (me.z == line - 1)
    inner_line = jnp.logical_not(ends_line)

    planes = [me.z, me.base + 1 - me.zp]
    for i in range(2, line, 2):
        pair = lax.rem(me.base + i, line)
        planes += [pair + me.zp, pair + 1 - me.zp]
    up_part = [pl.ds(h * (deep // 2), deep // 2) for h in range(2)]
    dn_part = [pl.ds(h * (hidden // 2), hidden // 2) for h in range(2)]

    def up_piece(z, h):
        lanes = pl.ds(pl.multiple_of((z % 2) * hidden, hidden), hidden)
        return wup_hbm.at[up_part[h], lanes]

    def dn_piece(z, h):
        at = (z % 2) * hidden + h * (hidden // 2)
        return wdn_hbm.at[pl.ds(pl.multiple_of(at, hidden // 2), hidden // 2), :]

    def send_up(z, h, cond=None):
        dst = up_s.at[me.sp, up_part[h]]
        start(wire.copy(up_piece(z, h), dst, up_z[h] + z, me.at(z=z), up_z[h] + me.z), cond)

    def send_dn(z, h, cond=None):
        dst = dn_s.at[me.sp, dn_part[h]]
        copy = wire.copy(dn_piece(z, h), dst, dn_z[h] + z, me.at(z=z), dn_z[h] + me.z)
        start(copy, cond)
        return copy

    beside = me.at(y=1 - me.y)

    def over_up(z, h, own=False):
        ref = up_s.at[z * 2 + me.y, up_part[h]]
        return wire.copy(up_piece(z, h) if own else ref, ref, up_y[h] + z, beside)

    def over_dn(z, h, own=False):
        ref = dn_s.at[z * 2 + me.y, dn_part[h]]
        return wire.copy(dn_piece(z, h) if own else ref, ref, dn_y[h] + z, beside)

    def relay_up(z, h):
        ref = up_s.at[z * 2 + me.y, up_part[h]]
        wire.copy(ref, ref, up_z[h] + z, me.at(z=z)).wait_recv()
        start(over_up(z, h))

    def crossed_up(z, h):
        ref = up_s.at[z * 2 + 1 - me.y, up_part[h]]
        wire.copy(ref, ref, up_y[h] + z, beside).wait_recv()

    def crossed_dn(z, h):
        ref = dn_s.at[z * 2 + 1 - me.y, dn_part[h]]
        wire.copy(ref, ref, dn_y[h] + z, beside).wait_recv()

    k_in = load(k_hbm, k_s, 0)
    v_in = load(v_hbm, v_s, 1)
    q_in = load(q_hbm, q_s, 2)
    og_in = load(og_hbm, og_s, 3)
    wo_in = load(wo_hbm, wo_s.at[me.tp], 4)
    res_in = load(res_hbm, res_s, 5)
    own_in = []
    for h in range(2):
        own_in.append(load(up_piece(me.z, h), up_s.at[me.sp, up_part[h]], 6 + h))
    dn_in = [load(dn_piece(me.z, h), dn_s.at[me.sp, dn_part[h]], 8 + h) for h in range(2)]

    barrier = pltpu.get_barrier_semaphore()
    met = [me.at(z=z) for z in planes[1:]]
    met += [beside, me.at(c=1 - me.c), me.at(x=1 - me.x), me.at(x=1 - me.x, c=1 - me.c)]
    met += [(lax.rem(me.sp + i, n_sp), me.tp) for i in (1, n_sp - 1)]
    for where in met:
        pl.semaphore_signal(barrier, inc=1, device_id=where, device_id_type=MESH)
    pl.semaphore_wait(barrier, len(met))
    send_up(planes[2], 0)
    send_up(planes[1], 0)
    start(over_up(me.z, 0, True))
    wo_no = [wire.slot() for _ in range(3)]
    core = me.at(c=1 - me.c)
    over = me.at(x=1 - me.x)
    above = me.at(z=me.base + 1 - me.zp)
    far_x, far_c = 1 - me.x, 1 - me.c

    def heads_row(number, where, owner_tp, src=None):
        ref = wo_s.at[owner_tp]
        return wire.copy(ref if src is None else src, ref, number, where)

    start(heads_row(wo_no[0], over, me.tp, wo_hbm))
    start(heads_row(wo_no[1], core, me.tp, wo_hbm))
    lane = lax.broadcasted_iota(jnp.int32, (8, length), 1)
    sub = lax.broadcasted_iota(jnp.int32, (8, length), 0)
    pre = jnp.concatenate([fg_ref[0], fg_ref[1]], axis=0)
    logf = jnp.minimum(pre, 0.0) - jnp.log1p(jnp.exp(-jnp.abs(pre)))
    cum_f = jnp.broadcast_to(logf[0:1], (8, length))
    cum_b = jnp.broadcast_to(logf[1:2], (8, length))
    step = 1
    while step < length:
        cum_f = cum_f + jnp.where(lane >= step, pltpu.roll(cum_f, step, 1), 0.0)
        cum_b = cum_b + jnp.where(lane < length - step, pltpu.roll(cum_b, length - step, 1), 0.0)
        step *= 2
    gate = jnp.concatenate([ig_ref[0], ig_ref[1]], axis=0)
    rel_f = jnp.broadcast_to(gate[0:1], (8, length)) - cum_f
    rel_b = jnp.broadcast_to(gate[1:2], (8, length)) - cum_b
    doc = jnp.broadcast_to(doc_ref[...].reshape(1, length).astype(f32), (8, length))
    total_f, total_b = cum_f[:, length - 1 :], cum_b[:, 0:1]
    first, last = doc[:, 0:1], doc[:, length - 1 :]
    exp_f = jnp.where(doc == last, total_f + rel_f, far_low)
    exp_b = jnp.where(doc == first, total_b + rel_b, far_low)
    peak_f = jnp.max(exp_f, axis=1, keepdims=True)
    peak_b = jnp.max(exp_b, axis=1, keepdims=True)
    keep_f, keep_b = jnp.exp(exp_f - peak_f), jnp.exp(exp_b - peak_b)
    rows_s[...] = jnp.where(sub == 0, rel_f, jnp.where(sub == 1, rel_b, doc))
    table = jnp.where(sub == 0, cum_f, cum_b)
    table = jnp.where(sub == 2, doc, table)
    table = jnp.where(sub == 3, keep_f, table)
    table = jnp.where(sub == 4, keep_b, table)
    cols_s[...] = table.T

    k_in.wait()
    v_in.wait()
    wide_keys = k_s[...].astype(f32)

    def own(d, column, peak, total, doc_out):
        weighted = (wide_keys * cols_s[:, column : column + 1]).astype(bf16)
        norm = jnp.sum(weighted.astype(f32), axis=0, keepdims=True)
        own_s[d] = lax.dot_general(
            weighted, v_s[...], (((0,), (0,)), ((), ())), preferred_element_type=f32
        ).astype(bf16)
        at = lax.broadcasted_iota(jnp.int32, (8, depth), 0)
        info = jnp.where(at == 0, jnp.broadcast_to(norm, (8, depth)), peak)
        info = jnp.where(at == 2, total, info)
        own_info_s[d] = jnp.where(at == 3, doc_out, info)

    own(0, 3, peak_f, total_f, last)
    own(1, 4, peak_b, total_b, first)

    def reach_of(d, far):
        sign = 1 if d == 0 else -1
        to, frm = me.sp + sign * far, me.sp - sign * far
        can_send = (to < n_sp) if d == 0 else (to >= 0)
        can_recv = (frm >= 0) if d == 0 else (frm < n_sp)
        return to, can_send, can_recv

    state_no = [[(wire.slot(), wire.slot()) for _ in range(2)] for _ in range(3)]

    def state_copies(r, d, far, src, info):
        to, can_send, can_recv = reach_of(d, far)
        to = jnp.clip(to, 0, n_sp - 1)
        a, b = state_no[r][d]
        return (
            wire.copy(src.at[d], got_s.at[r, d], a, (to, me.tp)),
            wire.copy(info.at[d], got_info_s.at[r, d], b, (to, me.tp)),
            can_send,
            can_recv,
        )

    def state_send(r, d, far, src, info):
        mem, note, can_send, can_recv = state_copies(r, d, far, src, info)
        start(note, can_send)
        start(mem, can_send)

        @pl.when(jnp.logical_not(can_recv))
        def _():
            got_s[r, d] = jnp.zeros(got_s.shape[2:], bf16)
            got_info_s[r, d] = jnp.full(got_info_s.shape[2:], -1.0, f32)

    def state_recv(r, d, far, src, info):
        mem, note, _, can_recv = state_copies(r, d, far, src, info)

        @pl.when(can_recv)
        def _():
            note.wait_recv()
            mem.wait_recv()

    for far in (1, 2):
        for d in (0, 1):
            state_send(far - 1, d, far, own_s, own_info_s)
    send_up(planes[2], 1)
    send_up(planes[1], 1)
    start(over_up(me.z, 1, True))

    q_in.wait()

    def inside(j, carry):
        r0 = pl.multiple_of(j * rows, rows)
        score = (
            lax.dot_general(
                q_s[pl.ds(r0, rows), :],
                k_s[...],
                (((1,), (1,)), ((), ())),
                preferred_element_type=f32,
            )
            * scale
        )
        at_row = lax.broadcasted_iota(jnp.int32, (rows, length), 0) + r0
        at_col = lax.broadcasted_iota(jnp.int32, (rows, length), 1)
        cols = cols_s[pl.ds(r0, rows), :]
        same = cols[:, 2:3] == rows_s[2:3, :]
        for d in (0, 1):
            order = (at_row >= at_col) if d == 0 else (at_row <= at_col)
            exponent = jnp.where(
                same & order, cols[:, d : d + 1] + rows_s[d : d + 1, :], far_low
            )
            top = jnp.max(exponent, axis=1, keepdims=True)
            weights = score * jnp.exp(exponent - top)
            stat_s[2 * d, pl.ds(r0, rows), :] = top
            stat_s[2 * d + 1, pl.ds(r0, rows), :] = jnp.sum(weights, axis=1, keepdims=True)
            num_s[d, pl.ds(r0, rows), :] = jnp.dot(
                weights.astype(bf16), v_s[...], preferred_element_type=f32
            )
        return carry

    lax.fori_loop(0, length // rows, inside, 0)

    def info_row(r, d, i):
        return got_info_s[r, d, i : i + 1, :]

    near = []
    for d in (0, 1):
        here = (first if d == 0 else last)[0:1]
        state_recv(0, d, 1, own_s, own_info_s)
        state_recv(1, d, 2, own_s, own_info_s)
        link1 = info_row(0, d, 3) == here
        link2 = info_row(1, d, 3) == here
        level1 = jnp.where(link1, info_row(0, d, 1), far_low)
        level2 = jnp.where(link2, info_row(1, d, 1) + info_row(0, d, 2), far_low)
        top = jnp.maximum(level1, level2)
        share1 = jnp.where(link1, jnp.exp(level1 - top), 0.0)
        share2 = jnp.where(link2, jnp.exp(level2 - top), 0.0)
        norm = share1 * info_row(0, d, 0) + share2 * info_row(1, d, 0)
        mid_s[d] = (
            share1[:, 0:1] * got_s[0, d].astype(f32) + share2[:, 0:1] * got_s[1, d].astype(f32)
        ).astype(bf16)
        at = lax.broadcasted_iota(jnp.int32, (8, depth), 0)
        mid_info_s[d] = jnp.where(at == 0, norm, jnp.where(at == 1, top, here))
        state_send(2, d, 2, mid_s, mid_info_s)
        near.append((here, top, norm))

    relay_up(planes[2], 0)
    relay_up(planes[1], 0)

    ends = []
    for d in (0, 1):
        here, top, norm = near[d]
        state_recv(2, d, 2, mid_s, mid_info_s)
        link = info_row(2, d, 3) == here
        level = jnp.where(
            link, info_row(2, d, 1) + info_row(1, d, 2) + info_row(0, d, 2), far_low
        )
        peak = jnp.maximum(top, level)
        link1 = info_row(0, d, 3) == here
        share = jnp.where(link1, jnp.exp(top - peak), 0.0)
        share_far = jnp.where(link, jnp.exp(level - peak), 0.0)
        fin_s[d] = (
            share[:, 0:1] * mid_s[d].astype(f32) + share_far[:, 0:1] * got_s[2, d].astype(f32)
        ).astype(bf16)
        meets = jnp.where(link1, here, -2.0)
        ends.append((meets[:, 0:1], peak, share * norm + share_far * info_row(2, d, 0)))

    for h in range(2):
        for i in range(3, line):
            send_up(planes[i], h)
    send_dn(planes[2], 0)
    og_in.wait()

    def project(j):
        r0 = pl.multiple_of(j * rows, rows)
        queries = q_s[pl.ds(r0, rows), :]
        wide_q = queries.astype(f32)
        cols = cols_s[pl.ds(r0, rows), :]
        memory = None
        for d in (0, 1):
            meets, level, norm = ends[d]
            usable = cols[:, 2:3] == meets
            carried = jnp.where(usable, cols[:, d : d + 1] + level[:, 0:1], far_low)
            top = stat_s[2 * d, pl.ds(r0, rows), :]
            peak = jnp.maximum(carried, top)
            local = jnp.exp(top - peak)
            inter = jnp.where(usable, jnp.exp(carried - peak), 0.0) * scale
            den = local * stat_s[2 * d + 1, pl.ds(r0, rows), :] + inter * jnp.sum(
                wide_q * norm, axis=1, keepdims=True
            )
            under = 1.0 / jnp.maximum(jnp.abs(den), 1.0)
            term = (local * under) * num_s[d, pl.ds(r0, rows), :] + (inter * under) * jnp.dot(
                queries, fin_s[d], preferred_element_type=f32
            )
            memory = term if memory is None else memory + term
        normed = memory * lax.rsqrt(jnp.mean(memory * memory, axis=1, keepdims=True) + eps)
        open_gate = jax.nn.sigmoid(og_s[pl.ds(r0, rows), :].astype(f32))
        read_s[j] = (normed * hg_ref[...].reshape(1, width) * open_gate).astype(bf16)

    ro_no = [wire.slot() for _ in range(3)]
    peers = [(far_x, far_c), (far_x, me.c), (me.x, far_c)]

    def exchange(i):
        x, c = peers[i]
        return wire.copy(read_s.at[x * 2 + c], heads_s.at[me.tp], ro_no[i], me.at(x=x, c=c))

    for i in range(3):
        project(peers[i][0] * 2 + peers[i][1])
        start(exchange(i))
    project(me.tp)
    relay_up(planes[1], 1)
    relay_up(planes[2], 1)
    who_wo = far_x * 2 + me.c
    heads_row(wo_no[0], over, who_wo).wait_recv()
    start(heads_row(wo_no[2], core, who_wo))
    res_in.wait()
    wo_in.wait()

    def head_part(rows_ref, owner_tp):
        part = jnp.dot(rows_ref[...], wo_s[owner_tp], preferred_element_type=f32)
        return part.astype(bf16).astype(f32)

    mixed_s[...] = res_s[...].astype(f32) + head_part(read_s.at[me.tp], me.tp)
    for i in (2, 1, 0):
        x, c = peers[i]
        frm = x * 2 + c
        if i == 2:
            heads_row(wo_no[1], core, frm).wait_recv()
        if i == 0:
            heads_row(wo_no[2], core, frm).wait_recv()
        wire.copy(read_s.at[me.tp], heads_s.at[frm], ro_no[i], me.at(x=x, c=c)).wait_recv()
        mixed_s[...] += head_part(heads_s.at[frm], frm)
    mixed = mixed_s[...]
    factor = lax.rsqrt(jnp.mean(mixed * mixed, axis=1, keepdims=True) + eps)
    mine = me.zp * n_tp + me.tp
    nrm_s[mine] = (mixed * factor * ng_ref[...].reshape(1, nrm_s.shape[2])).astype(bf16)

    inner = jnp.where(me.base == 0, 1, me.base)
    others = [
        jnp.where(me.base == 0, 2 + i, lax.rem(me.base + line - 1 - i, line))
        for i in range(line - 2)
    ]
    course = [inner, 2 * me.base + 1 - inner] + others
    order = []
    for z in course:
        order += [(z, me.y), (z, 1 - me.y)]

    def relay_dn(z, h, cond=None):
        ref = dn_s.at[z * 2 + me.y, dn_part[h]]
        got = wire.copy(ref, ref, dn_z[h] + z, me.at(z=z))
        if cond is None:
            got.wait_recv()
        else:
            pl.when(cond)(got.wait_recv)
        start(over_dn(z, h), cond)

    def owner(zp, x, c):
        return zp * n_tp + x * 2 + c

    far_z = 1 - me.zp
    n_core = [wire.slot() for _ in range(2)]
    n_x = wire.slot()
    n_z, n_xz = [wire.slot(), wire.slot()], [wire.slot(), wire.slot()]
    n_corez, n_corexz = [wire.slot(), wire.slot()], [wire.slot(), wire.slot()]
    half = rows // 2
    parts = [pl.ds(0, half), pl.ds(half, half)]

    def pass_on(number, where, who, part=None):
        ref = nrm_s.at[who] if part is None else nrm_s.at[who, part]
        return wire.copy(ref, ref, number, where)

    start(pass_on(n_x, over, mine))
    for h in range(2):
        start(pass_on(n_z[h], above, mine, parts[h]))
    start(pass_on(n_core[0], core, mine))
    near_dn = [send_dn(planes[1], h) for h in range(2)]
    for h in range(2):
        start(over_dn(me.z, h, True))
    for h in range(2):
        for i in range(3, line):
            relay_up(planes[i], h)

    def raise_rows(zp, x):
        group = zp * 2 + x

        def chunk(n, carry):
            c0 = pl.multiple_of(n * 256, 256)
            left = nrm_s[pl.ds(group * 2, 2), :, :].reshape(2 * rows, nrm_s.shape[2])
            right = up_s[:, :, pl.ds(c0, 256)].reshape(n_sp * deep, 256)
            pre = jnp.maximum(jnp.dot(left, right, preferred_element_type=f32), 0.0)
            hid_s[group, :, pl.ds(c0, 256)] = (pre * pre).astype(bf16)
            return carry

        lax.fori_loop(0, hidden // 256, chunk, 0)

    who = owner(me.zp, far_x, me.c)
    pass_on(n_x, over, who).wait_recv()
    start(pass_on(n_core[1], core, who))
    for h in range(2):
        for i in range(3, line):
            send_dn(planes[i], h, inner_line)
    relay_dn(planes[2], 0)
    who = owner(far_z, me.x, me.c)
    for h in range(2):
        pass_on(n_z[h], above, who, parts[h]).wait_recv()
        start(pass_on(n_xz[h], over, who, parts[h]))
        start(pass_on(n_corez[h], core, who, parts[h]))
    for copy in own_in:
        copy.wait()
    for z in planes:
        for h in range(2):
            crossed_up(z, h)
    pass_on(n_core[0], core, owner(me.zp, me.x, far_c)).wait_recv()
    raise_rows(me.zp, me.x)
    pass_on(n_core[1], core, owner(me.zp, far_x, far_c)).wait_recv()
    raise_rows(me.zp, far_x)
    for h in range(2):
        pass_on(n_corez[h], core, owner(far_z, me.x, far_c), parts[h]).wait_recv()
    raise_rows(far_z, me.x)
    for copy in near_dn:
        drain(copy)
    send_dn(planes[2], 1)
    for h in range(2):
        relay_dn(planes[1], h)
    who = owner(far_z, far_x, me.c)
    for h in range(2):
        pass_on(n_xz[h], over, who, parts[h]).wait_recv()
        start(pass_on(n_corexz[h], core, who, parts[h]))
    for h in range(2):
        pass_on(n_corexz[h], core, owner(far_z, far_x, far_c), parts[h]).wait_recv()
    raise_rows(far_z, far_x)
    for copy in dn_in:
        copy.wait()

    blocks = n_sp
    r1_no = [wire.slot() for _ in range(blocks)]
    r2_no = [wire.slot() for _ in range(blocks)]
    r3_no = [wire.slot() for _ in range(blocks)]
    groups = 4

    def lower(k):
        z, y = order[k]
        if k == 0:
            for h in range(2):
                for i in range(3, line):
                    send_dn(planes[i], h, ends_line)
        if k == 1:
            for h in range(2):
                for i in range(3, line):
                    relay_dn(planes[i], h, inner_line)
        if k == 3:
            relay_dn(planes[2], 1)
        if k in (4, 5):
            for i in range(3, line):
                relay_dn(planes[i], k - 4, ends_line)
        if k % 2 == 1:
            for h in range(2):
                crossed_dn(z, h)
        slot = z * 2 + y

        def one(g, carry):
            value = jnp.dot(hid_s[g], dn_s[slot], preferred_element_type=f32).astype(bf16)
            part_s[k, 0, g] = value[:rows]
            part_s[k, 1, g] = value[rows:]
            return carry

        lax.fori_loop(0, groups, one, 0)
        start(wire.copy(part_s.at[k, far_c], r1_s.at[k], r1_no[k], core))

    def over_x(k):
        return k < blocks // 2 or k % 2 == 1

    def sum1(k):
        wire.copy(part_s.at[k, far_c], r1_s.at[k], r1_no[k], core).wait_recv()

        def both(g):
            return part_s[k, me.c, g].astype(f32) + r1_s[k, g].astype(f32)

        for i in range(2):
            away = i * 2 + far_x if over_x(k) else far_z * 2 + i
            r2_out_s[k, i] = both(away).astype(bf16)
        start(wire.copy(r2_out_s.at[k], r2_in_s.at[k], r2_no[k], over if over_x(k) else above))
        for i in range(2):
            here = i * 2 + me.x if over_x(k) else me.zp * 2 + i
            r2_keep_s[k, i] = both(here)

    def sum2(k):
        first, second = (over, above) if over_x(k) else (above, over)
        wire.copy(r2_out_s.at[k], r2_in_s.at[k], r2_no[k], first).wait_recv()
        far = far_z if over_x(k) else far_x
        r3_out_s[k] = (r2_keep_s[k, far] + r2_in_s[k, far].astype(f32)).astype(bf16)
        start(wire.copy(r3_out_s.at[k], r3_in_s.at[k], r3_no[k], second))

    def sum3(k):
        second = above if over_x(k) else over
        wire.copy(r3_out_s.at[k], r3_in_s.at[k], r3_no[k], second).wait_recv()
        z, y = order[k]
        c0 = pl.multiple_of((z * 2 + y) * wide, wide)
        at = me.zp if over_x(k) else me.x
        total = r2_keep_s[k, at] + r2_in_s[k, at].astype(f32) + r3_in_s[k].astype(f32)
        total = mixed_s[:, pl.ds(c0, wide)] + total
        out_ref[:, pl.ds(c0, wide)] = total.astype(bf16)

    for k in range(blocks + 4):
        if 0 <= k - 1 < blocks:
            sum1(k - 1)
        if k < blocks:
            lower(k)
        if 0 <= k - 2 < blocks:
            sum2(k - 2)
        if 0 <= k - 4 < blocks:
            sum3(k - 4)

    for copy, cond in waits:
        if cond is None:
            copy.wait_send()
        else:
            pl.when(cond)(copy.wait_send)


def fused(n_sp, n_tp, *args):
    (
        queries,
        keys,
        values,
        out_gate,
        input_gates,
        forget_gates,
        doc_ids,
        head_gain,
        w_out,
        resid,
        norm_gain,
        w_up,
        w_down,
    ) = args
    length, depth = queries.shape
    width = values.shape[1]
    rows, model = resid.shape
    deep, wide = w_up.shape[0], w_down.shape[1]
    hidden = w_up.shape[1] // 2
    line = n_sp // 2
    blocks = n_sp
    numbers = 8 * line + 32 + 3 * blocks
    vmem = pltpu.VMEM
    scratch = [
        vmem((length, depth), bf16),
        vmem((length, depth), bf16),
        vmem((length, width), bf16),
        vmem((length, width), bf16),
        vmem((n_tp, width, model), bf16),
        vmem((rows, model), bf16),
        vmem((n_sp, deep, hidden), bf16),
        vmem((n_sp, hidden, wide), bf16),
        vmem((8, length), f32),
        vmem((length, 8), f32),
        vmem((2, length, width), f32),
        vmem((4, length, 1), f32),
        vmem((2, depth, width), bf16),
        vmem((2, 8, depth), f32),
        vmem((3, 2, depth, width), bf16),
        vmem((3, 2, 8, depth), f32),
        vmem((2, depth, width), bf16),
        vmem((2, 8, depth), f32),
        vmem((2, depth, width), bf16),
        vmem((n_tp, rows, width), bf16),
        vmem((n_tp, rows, width), bf16),
        vmem((rows, model), f32),
        vmem((2 * n_tp, rows, model), bf16),
        vmem((4, 2 * rows, hidden), bf16),
        vmem((blocks, 2, 4, rows, wide), bf16),
        vmem((blocks, 4, rows, wide), bf16),
        vmem((blocks, 2, rows, wide), bf16),
        vmem((blocks, 2, rows, wide), f32),
        vmem((blocks, 2, rows, wide), bf16),
        vmem((blocks, rows, wide), bf16),
        vmem((blocks, rows, wide), bf16),
        pltpu.SemaphoreType.DMA((10,)),
        pltpu.SemaphoreType.DMA((numbers,)),
        pltpu.SemaphoreType.DMA((numbers,)),
    ]
    anywhere = pl.BlockSpec(memory_space=pl.ANY)
    inside = pl.BlockSpec(memory_space=pltpu.VMEM)
    return pl.pallas_call(
        functools.partial(layer_kernel, n_sp, n_tp),
        out_shape=jax.ShapeDtypeStruct((rows, model), bf16),
        in_specs=[anywhere] * 4 + [inside] * 4 + [anywhere] * 2 + [inside] + [anywhere] * 2,
        out_specs=inside,
        scratch_shapes=scratch,
        compiler_params=pltpu.CompilerParams(
            collective_id=0, has_side_effects=True, vmem_limit_bytes=66_000_000
        ),
        name="layer",
    )(
        queries,
        keys,
        values,
        out_gate,
        input_gates,
        forget_gates,
        doc_ids,
        head_gain,
        w_out,
        resid,
        norm_gain,
        w_up,
        w_down,
    )


def fits(mesh, args):
    n_sp, n_tp = mesh.shape["sp"], mesh.shape["tp"]
    queries, input_gates, w_up, w_down = args[0], args[4], args[11], args[12]
    length = queries.shape[0] // n_sp
    return (
        n_tp == 4
        and n_sp % 4 == 0
        and input_gates.shape[1] == n_tp
        and -(-longest_doc // length) <= 4
        and length % (n_tp * 32) == 0
        and w_down.shape[1] % (n_sp * 128) == 0
        and w_up.shape[0] % (n_sp * 16) == 0
        and w_up.shape[1] % (n_tp * 512) == 0
    )


def solution(mesh):
    in_specs = (
        P("sp", "tp"),
        P("sp", "tp"),
        P("sp", "tp"),
        P("sp", "tp"),
        P(None, "tp", "sp"),
        P(None, "tp", "sp"),
        P("sp"),
        P("tp"),
        P("tp", None),
        P(("sp", "tp"), None),
        P(),
        P("sp", "tp"),
        P("tp", "sp"),
    )
    out_specs = P(("sp", "tp"), None)

    def step(*args):
        whole = fits(mesh, args)
        body = functools.partial(fused, mesh.shape["sp"], mesh.shape["tp"]) if whole else shards
        return jax.shard_map(
            body, mesh=mesh, in_specs=in_specs, out_specs=out_specs, check_vma=False
        )(*args)

    return step
```

```python
import functools

import jax
import jax.numpy as jnp
from jax import lax
from jax.experimental import pallas as pl
from jax.experimental.pallas import tpu as pltpu
from jax.sharding import PartitionSpec as P


eps = 1e-06
far_low = -1e30
longest_doc = 3072


MESH = pl.DeviceIdType.MESH
bf16 = jnp.bfloat16
f32 = jnp.float32


def dot(a, b):
    return jnp.dot(a, b, preferred_element_type=f32)


class Lines:
    def __init__(self):
        count = lax.axis_size("sp")
        self.pair = 2 if count % 2 == 0 else 1
        self.line = count // self.pair

    def along(self, value, step):
        table = [
            (z * self.pair + y, (z + step) * self.pair + y)
            for z in range(self.line)
            for y in range(self.pair)
            if 0 <= z + step < self.line
        ]
        return lax.ppermute(value, "sp", table)

    def across(self, value, valid):
        table = [
            (z * self.pair + y, z * self.pair + 1 - y)
            for z in range(self.line)
            if valid(z)
            for y in range(self.pair)
        ]
        return lax.ppermute(value, "sp", table)

    def order(self):
        place = lax.axis_index("sp")
        z, y = place // self.pair, place % self.pair
        sources = []
        for k in range(self.line):
            row = (z + self.line - k) % self.line
            sources.append(row * self.pair + y)
            if self.pair == 2:
                sources.append(row * self.pair + 1 - y)
        return jnp.stack(sources)

    def piece(self, source):
        place = lax.axis_index("sp")
        z, y = place // self.pair, place % self.pair
        k = (z + self.line - source // self.pair) % self.line
        return k * self.pair + (y + source) % self.pair

    def gather(self, own):
        n = self.line
        up, down = {}, {}
        up_side, down_side = {}, {}
        two = self.pair == 2
        own_side = self.across(own, lambda z: True) if two else None
        prev_up = prev_down = own
        for k in range(1, n):
            prev_up = up[k] = self.along(prev_up, 1)
            prev_down = down[k] = self.along(prev_down, -1)
            if two:
                up_side[k] = self.across(prev_up, lambda z: z >= k)
                down_side[k] = self.across(prev_down, lambda z: z + k < n)
        groups = [[own] + ([own_side] if two else [])]
        z = lax.axis_index("sp") // self.pair
        for k in range(1, n):
            below = z >= k
            group = [jnp.where(below, up[k], down[n - k])]
            if two:
                group.append(jnp.where(below, up_side[k], down_side[n - k]))
            groups.append(group)
        return groups


class Heads:
    def __init__(self):
        count = lax.axis_size("tp")
        self.core = 2 if count % 2 == 0 else 1
        self.far = count // self.core

    def swap(self, value):
        count = lax.axis_size("tp")
        return lax.ppermute(value, "tp", [(i, i ^ 1) for i in range(count)])

    def shift(self, value, step):
        table = [
            (x * self.core + c, ((x + step) % self.far) * self.core + c)
            for x in range(self.far)
            for c in range(self.core)
        ]
        return lax.ppermute(value, "tp", table)

    def gather(self, own):
        mine = [own] + [self.shift(own, r) for r in range(1, self.far)]
        if self.core == 1:
            return jnp.concatenate(mine)
        return jnp.concatenate(mine + [self.swap(block) for block in mine])

    def reduce(self, near, away):
        total = near.astype(f32)
        if away is not None:
            total = total + self.swap(away).astype(f32)
        out = total[0]
        for r in range(1, self.far):
            out = out + self.shift(total[r].astype(bf16), -r).astype(f32)
        return out


def local_part(scores, values, exponent, keep):
    top = jnp.max(jnp.where(keep, exponent, far_low), axis=1)
    weights = jnp.where(keep, scores * jnp.exp(exponent - top[:, None]), 0.0)
    return top, dot(weights.astype(bf16), values), jnp.sum(weights, axis=1)


def summary(keys, exponent):
    peak = jnp.max(exponent)
    weighted = (keys * jnp.exp(exponent - peak)[:, None]).astype(bf16)
    return weighted, jnp.sum(weighted.astype(f32), axis=0), peak


def split_row(row, width):
    terms, rest = [], row
    for _ in range(3):
        term = lax.reduce_precision(rest, 8, 7)
        rest = rest - term
        terms.append(term.astype(bf16))
    lines = -(-row.shape[0] // width)
    table = jnp.stack([jnp.pad(t, (0, lines * width - t.shape[0])) for t in terms])
    table = table.reshape(3 * lines, width)
    return jnp.pad(table, ((0, -(3 * lines) % 16), (0, 0)))


def join_row(table, size):
    lines = -(-size // table.shape[1])
    terms = table[: 3 * lines].astype(f32).reshape(3, -1)
    return (terms[0] + terms[1] + terms[2])[:size]


def incoming(memory, row, doc_here, sign, reach):
    count = lax.axis_size("sp")
    place = lax.axis_index("sp")
    depth, width = memory.shape
    sent = jnp.concatenate([memory, split_row(row, width)])
    arrived = []
    for d in range(1, min(reach, count - 1) + 1):
        table = [(i, i + sign * d) for i in range(count) if 0 <= i + sign * d < count]
        got = lax.ppermute(sent, "sp", table)
        arrived.append((join_row(got[depth:], row.shape[0]), got[:depth]))
    passed = jnp.zeros((), f32)
    levels, linked = [], []
    for d, (got, _) in enumerate(arrived, 1):
        there = (place >= d) if sign > 0 else (place + d < count)
        joined = there & (got[depth + 2] == doc_here)
        levels.append(jnp.where(joined, got[depth] + passed, far_low))
        linked.append(joined)
        passed = passed + got[depth + 1]
    top = jnp.max(jnp.stack(levels))
    state = jnp.zeros(memory.shape, f32)
    norm = jnp.zeros((depth,), f32)
    for level, joined, (got, mem) in zip(levels, linked, arrived):
        share = jnp.where(joined, jnp.exp(level - top), 0.0)
        state = state + share * mem.astype(f32)
        norm = norm + share * got[:depth]
    return state.astype(bf16), norm, top, linked[0]


def one_head(queries, keys, values, in_gates, forget_pre, doc_pos, reach):
    length, depth = queries.shape
    scale = depth ** (-0.5)
    place = jnp.arange(length)
    logf = jax.nn.log_sigmoid(forget_pre)
    before = place[:, None] >= place[None, :]
    after = place[:, None] <= place[None, :]
    cum_f = jnp.sum(jnp.where(before, logf[0][None, :], 0.0), axis=1)
    cum_b = jnp.sum(jnp.where(after, logf[1][None, :], 0.0), axis=1)
    total_f, total_b = cum_f[length - 1], cum_b[0]
    first, last = doc_pos[0], doc_pos[length - 1]
    weighted_f, norm_f, peak_f = summary(
        keys, jnp.where(doc_pos == last, total_f - cum_f + in_gates[0], far_low)
    )
    weighted_b, norm_b, peak_b = summary(
        keys, jnp.where(doc_pos == first, total_b - cum_b + in_gates[1], far_low)
    )

    def own_state(weighted):
        return lax.dot_general(
            weighted, values, (((0,), (0,)), ((), ())), preferred_element_type=f32
        ).astype(bf16)

    pad = jnp.zeros((125,), f32)
    row_f = jnp.concatenate([norm_f, jnp.stack([peak_f, total_f, last]), pad])
    row_b = jnp.concatenate([norm_b, jnp.stack([peak_b, total_b, first]), pad])
    state_f, norm_in_f, top_f, has_f = incoming(own_state(weighted_f), row_f, first, 1, reach)
    state_b, norm_in_b, top_b, has_b = incoming(own_state(weighted_b), row_b, last, -1, reach)

    scores = (
        lax.dot_general(queries, keys, (((1,), (1,)), ((), ())), preferred_element_type=f32) * scale
    )
    same = doc_pos[:, None] == doc_pos[None, :]
    wide = queries.astype(f32)

    def finish(cum, gate, keep, state, norm_in, top_in, usable):
        exponent = cum[:, None] - cum[None, :] + gate[None, :]
        top, numer, denom = local_part(scores, values, exponent, keep)
        carried = jnp.where(usable, cum + top_in, far_low)
        peak = jnp.maximum(carried, top)
        local = jnp.exp(top - peak)
        inter = jnp.where(usable, jnp.exp(carried - peak), 0.0) * scale
        denom = local * denom + inter * jnp.sum(wide * norm_in[None, :], axis=1)
        under = 1.0 / jnp.maximum(jnp.abs(denom), 1.0)
        return (local * under)[:, None] * numer + (inter * under)[:, None] * dot(queries, state)

    return finish(
        cum_f, in_gates[0], before & same, state_f, norm_in_f, top_f, has_f & (doc_pos == first)
    ) + finish(
        cum_b, in_gates[1], after & same, state_b, norm_in_b, top_b, has_b & (doc_pos == last)
    )


def pack(w_up, w_down):
    wide = w_down.shape[1]
    count = w_up.shape[1] // wide
    tiles = [w_down[i * wide : (i + 1) * wide] for i in range(count)]
    return jnp.concatenate([w_up, jnp.concatenate(tiles, axis=1)])


def unpack(table, wide):
    count = table.shape[1] // wide
    return jnp.concatenate([table[:, i * wide : (i + 1) * wide] for i in range(count)])


def shards(*args):
    return layer(*args)


def layer(
    queries,
    keys,
    values,
    out_gate,
    input_gates,
    forget_gates,
    doc_ids,
    head_gain,
    w_out,
    resid,
    norm_gain,
    w_up,
    w_down,
):
    length = queries.shape[0]
    heads = input_gates.shape[1]
    depth, width = queries.shape[1] // heads, values.shape[1] // heads
    lines, tps = Lines(), Heads()
    rows = resid.shape[0]
    doc_pos = doc_ids.astype(f32)
    reach = -(-longest_doc // length)
    deep_up, wide_down = w_up.shape[0], w_down.shape[1]
    groups = lines.gather(pack(w_up, w_down))
    ups = [[piece[:deep_up] for piece in group] for group in groups]
    downs = [[unpack(piece[deep_up:], wide_down) for piece in group] for group in groups]
    order = lines.order()

    parts = []
    for h in range(heads):
        at_k, at_v = slice(h * depth, (h + 1) * depth), slice(h * width, (h + 1) * width)
        memory = one_head(
            queries[:, at_k],
            keys[:, at_k],
            values[:, at_v],
            input_gates[:, h],
            forget_gates[:, h],
            doc_pos,
            reach,
        )
        normed = memory * lax.rsqrt(jnp.mean(memory * memory, axis=-1, keepdims=True) + eps)
        gate = jax.nn.sigmoid(out_gate[:, at_v].astype(f32))
        parts.append((normed * head_gain[at_v] * gate).astype(bf16))
    readout = parts[0] if heads == 1 else jnp.concatenate(parts, axis=1)

    projected = dot(readout, w_out).astype(bf16).reshape(tps.far, tps.core, rows, -1)
    me = lax.axis_index("tp")
    x, c = me // tps.core, me % tps.core

    def for_core(core):
        picked = lax.dynamic_index_in_dim(projected, core, 1, False)
        return jnp.stack(
            [
                lax.dynamic_index_in_dim(picked, (x + tps.far - r) % tps.far, 0, False)
                for r in range(tps.far)
            ]
        )

    summed = tps.reduce(for_core(c), for_core(1 - c) if tps.core == 2 else None)
    mixed = resid.astype(f32) + summed
    factor = lax.rsqrt(jnp.mean(mixed * mixed, axis=-1, keepdims=True) + eps)
    scaled = (mixed * factor * norm_gain).astype(bf16)

    blocks = order.shape[0]
    deep = scaled.shape[1] // blocks
    turned = jnp.concatenate(
        [lax.dynamic_slice_in_dim(scaled, order[i] * deep, deep, 1) for i in range(blocks)], axis=1
    )
    up_full = jnp.concatenate([piece for group in ups for piece in group], axis=0)
    product = dot(tps.gather(turned), up_full)
    hidden = jnp.square(jax.nn.relu(product)).astype(bf16)

    bundle = max(1, len(downs) // 4)
    outs = []
    for at in range(0, len(downs), bundle):
        pieces = [piece for group in downs[at : at + bundle] for piece in group]
        part = dot(hidden, jnp.concatenate(pieces, axis=1)).astype(bf16)
        part = part.reshape(tps.core, tps.far, rows, -1)
        outs.append(tps.reduce(part[0], part[1] if tps.core == 2 else None))
    summed = jnp.concatenate(outs, axis=1)
    back = jnp.concatenate(
        [lax.dynamic_slice_in_dim(summed, lines.piece(i) * deep, deep, 1) for i in range(blocks)],
        axis=1,
    )
    return (mixed + back).astype(bf16)


class Spot:
    def __init__(self, n_sp, n_tp):
        self.n_sp, self.n_tp = n_sp, n_tp
        self.line = n_sp // 2
        self.sp = lax.axis_index("sp")
        self.tp = lax.axis_index("tp")
        self.z, self.y = self.sp // 2, self.sp % 2
        self.x, self.c = self.tp // 2, self.tp % 2
        self.zp = self.z % 2
        self.base = self.z - self.zp

    def at(self, z=None, y=None, x=None, c=None):
        z = self.z if z is None else z
        y = self.y if y is None else y
        x = self.x if x is None else x
        c = self.c if c is None else c
        return (z * 2 + y, x * 2 + c)


class Wire:
    def __init__(self, send_sems, recv_sems):
        self.send_sems, self.recv_sems = send_sems, recv_sems
        self.count = 0

    def slot(self):
        self.count += 1
        return self.count - 1

    def copy(self, src, dst, number, where, arrival=None):
        return pltpu.make_async_remote_copy(
            src_ref=src,
            dst_ref=dst,
            send_sem=self.send_sems.at[number],
            recv_sem=self.recv_sems.at[number if arrival is None else arrival],
            device_id=where,
            device_id_type=MESH,
        )


def layer_kernel(
    n_sp,
    n_tp,
    q_hbm,
    k_hbm,
    v_hbm,
    og_hbm,
    ig_ref,
    fg_ref,
    doc_ref,
    hg_ref,
    wo_hbm,
    res_hbm,
    ng_ref,
    wup_hbm,
    wdn_hbm,
    out_ref,
    q_s,
    k_s,
    v_s,
    og_s,
    wo_s,
    res_s,
    up_s,
    dn_s,
    rows_s,
    cols_s,
    num_s,
    stat_s,
    own_s,
    own_info_s,
    got_s,
    got_info_s,
    mid_s,
    mid_info_s,
    fin_s,
    read_s,
    heads_s,
    mixed_s,
    nrm_s,
    hid_s,
    part_s,
    r1_s,
    r2_out_s,
    r2_keep_s,
    r2_in_s,
    r3_out_s,
    r3_in_s,
    local_sem,
    send_sem,
    recv_sem,
):
    me = Spot(n_sp, n_tp)
    wire = Wire(send_sem, recv_sem)
    line = me.line
    length, depth = q_s.shape
    width = v_s.shape[1]
    rows = res_s.shape[0]
    deep = wup_hbm.shape[0]
    hidden = up_s.shape[2]
    wide = wdn_hbm.shape[1]
    scale = depth ** (-0.5)
    waits = []

    def start(copy, cond=None):
        if cond is None:
            copy.start()
            waits.append((copy, None))
        else:
            pl.when(cond)(copy.start)
            waits.append((copy, cond))

    def load(src, dst, number):
        copy = pltpu.make_async_copy(src, dst, local_sem.at[number])
        copy.start()
        return copy

    up_z = [[wire.slot() for _ in range(line)][0] for _ in range(2)]
    dn_z = [[wire.slot() for _ in range(line)][0] for _ in range(2)]
    up_y = [[wire.slot() for _ in range(line)][0] for _ in range(2)]
    dn_y = [[wire.slot() for _ in range(line)][0] for _ in range(2)]
    ends_line = (me.z == 0) | (me.z == line - 1)
    inner_line = jnp.logical_not(ends_line)

    planes = [me.z, me.base + 1 - me.zp]
    for i in range(2, line, 2):
        pair = lax.rem(me.base + i, line)
        planes += [pair + me.zp, pair + 1 - me.zp]
    up_part = [pl.ds(h * (deep // 2), deep // 2) for h in range(2)]
    dn_part = [pl.ds(h * (hidden // 2), hidden // 2) for h in range(2)]

    def up_piece(z, h):
        lanes = pl.ds(pl.multiple_of((z % 2) * hidden, hidden), hidden)
        return wup_hbm.at[up_part[h], lanes]

    def dn_piece(z, h):
        at = (z % 2) * hidden + h * (hidden // 2)
        return wdn_hbm.at[pl.ds(pl.multiple_of(at, hidden // 2), hidden // 2), :]

    def send_up(z, h, cond=None):
        dst = up_s.at[me.sp, up_part[h]]
        start(wire.copy(up_piece(z, h), dst, up_z[h] + z, me.at(z=z), up_z[h] + me.z), cond)

    def send_dn(z, h, cond=None):
        dst = dn_s.at[me.sp, dn_part[h]]
        copy = wire.copy(dn_piece(z, h), dst, dn_z[h] + z, me.at(z=z), dn_z[h] + me.z)
        start(copy, cond)
        return copy

    beside = me.at(y=1 - me.y)

    def over_up(z, h, own=False):
        ref = up_s.at[z * 2 + me.y, up_part[h]]
        return wire.copy(up_piece(z, h) if own else ref, ref, up_y[h] + z, beside)

    def over_dn(z, h, own=False):
        ref = dn_s.at[z * 2 + me.y, dn_part[h]]
        return wire.copy(dn_piece(z, h) if own else ref, ref, dn_y[h] + z, beside)

    def relay_up(z, h):
        ref = up_s.at[z * 2 + me.y, up_part[h]]
        wire.copy(ref, ref, up_z[h] + z, me.at(z=z)).wait_recv()
        start(over_up(z, h))

    def crossed_up(z, h):
        ref = up_s.at[z * 2 + 1 - me.y, up_part[h]]
        wire.copy(ref, ref, up_y[h] + z, beside).wait_recv()

    def crossed_dn(z, h):
        ref = dn_s.at[z * 2 + 1 - me.y, dn_part[h]]
        wire.copy(ref, ref, dn_y[h] + z, beside).wait_recv()

    k_in = load(k_hbm, k_s, 0)
    v_in = load(v_hbm, v_s, 1)
    q_in = load(q_hbm, q_s, 2)
    og_in = load(og_hbm, og_s, 3)
    wo_in = load(wo_hbm, wo_s.at[me.tp], 4)
    res_in = load(res_hbm, res_s, 5)
    own_in = []
    for h in range(2):
        own_in.append(load(up_piece(me.z, h), up_s.at[me.sp, up_part[h]], 6 + h))
    dn_in = [load(dn_piece(me.z, h), dn_s.at[me.sp, dn_part[h]], 8 + h) for h in range(2)]

    barrier = pltpu.get_barrier_semaphore()
    met = [me.at(z=z) for z in planes[1:]]
    met += [beside, me.at(c=1 - me.c), me.at(x=1 - me.x), me.at(x=1 - me.x, c=1 - me.c)]
    met += [(lax.rem(me.sp + i, n_sp), me.tp) for i in (1, n_sp - 1)]
    for where in met:
        pl.semaphore_signal(barrier, inc=1, device_id=where, device_id_type=MESH)
    pl.semaphore_wait(barrier, len(met))
    send_up(planes[2], 0)
    send_up(planes[1], 0)
    start(over_up(me.z, 0, True))
    wo_no = [wire.slot() for _ in range(3)]
    core = me.at(c=1 - me.c)
    over = me.at(x=1 - me.x)
    above = me.at(z=me.base + 1 - me.zp)
    far_x, far_c = 1 - me.x, 1 - me.c

    def heads_row(number, where, owner_tp, src=None):
        ref = wo_s.at[owner_tp]
        return wire.copy(ref if src is None else src, ref, number, where)

    start(heads_row(wo_no[0], over, me.tp, wo_hbm))
    start(heads_row(wo_no[1], core, me.tp, wo_hbm))
    lane = lax.broadcasted_iota(jnp.int32, (8, length), 1)
    sub = lax.broadcasted_iota(jnp.int32, (8, length), 0)
    pre = jnp.concatenate([fg_ref[0], fg_ref[1]], axis=0)
    logf = jnp.minimum(pre, 0.0) - jnp.log1p(jnp.exp(-jnp.abs(pre)))
    cum_f = jnp.broadcast_to(logf[0:1], (8, length))
    cum_b = jnp.broadcast_to(logf[1:2], (8, length))
    step = 1
    while step < length:
        cum_f = cum_f + jnp.where(lane >= step, pltpu.roll(cum_f, step, 1), 0.0)
        cum_b = cum_b + jnp.where(lane < length - step, pltpu.roll(cum_b, length - step, 1), 0.0)
        step *= 2
    gate = jnp.concatenate([ig_ref[0], ig_ref[1]], axis=0)
    rel_f = jnp.broadcast_to(gate[0:1], (8, length)) - cum_f
    rel_b = jnp.broadcast_to(gate[1:2], (8, length)) - cum_b
    doc = jnp.broadcast_to(doc_ref[...].reshape(1, length).astype(f32), (8, length))
    total_f, total_b = cum_f[:, length - 1 :], cum_b[:, 0:1]
    first, last = doc[:, 0:1], doc[:, length - 1 :]
    exp_f = jnp.where(doc == last, total_f + rel_f, far_low)
    exp_b = jnp.where(doc == first, total_b + rel_b, far_low)
    peak_f = jnp.max(exp_f, axis=1, keepdims=True)
    peak_b = jnp.max(exp_b, axis=1, keepdims=True)
    keep_f, keep_b = jnp.exp(exp_f - peak_f), jnp.exp(exp_b - peak_b)
    rows_s[...] = jnp.where(sub == 0, rel_f, jnp.where(sub == 1, rel_b, doc))
    table = jnp.where(sub == 0, cum_f, cum_b)
    table = jnp.where(sub == 2, doc, table)
    table = jnp.where(sub == 3, keep_f, table)
    table = jnp.where(sub == 4, keep_b, table)
    cols_s[...] = table.T

    k_in.wait()
    v_in.wait()
    wide_keys = k_s[...].astype(f32)

    def own(d, column, peak, total, doc_out):
        weighted = (wide_keys * cols_s[:, column : column + 1]).astype(bf16)
        norm = jnp.sum(weighted.astype(f32), axis=0, keepdims=True)
        own_s[d] = lax.dot_general(
            weighted, v_s[...], (((0,), (0,)), ((), ())), preferred_element_type=f32
        ).astype(bf16)
        at = lax.broadcasted_iota(jnp.int32, (8, depth), 0)
        info = jnp.where(at == 0, jnp.broadcast_to(norm, (8, depth)), peak)
        info = jnp.where(at == 2, total, info)
        own_info_s[d] = jnp.where(at == 3, doc_out, info)

    own(0, 3, peak_f, total_f, last)
    own(1, 4, peak_b, total_b, first)

    def reach_of(d, far):
        sign = 1 if d == 0 else -1
        to, frm = me.sp + sign * far, me.sp - sign * far
        can_send = (to < n_sp) if d == 0 else (to >= 0)
        can_recv = (frm >= 0) if d == 0 else (frm < n_sp)
        return to, can_send, can_recv

    state_no = [[(wire.slot(), wire.slot()) for _ in range(2)] for _ in range(3)]

    def state_copies(r, d, far, src, info):
        to, can_send, can_recv = reach_of(d, far)
        to = jnp.clip(to, 0, n_sp - 1)
        a, b = state_no[r][d]
        return (
            wire.copy(src.at[d], got_s.at[r, d], a, (to, me.tp)),
            wire.copy(info.at[d], got_info_s.at[r, d], b, (to, me.tp)),
            can_send,
            can_recv,
        )

    def state_send(r, d, far, src, info):
        mem, note, can_send, can_recv = state_copies(r, d, far, src, info)
        start(note, can_send)
        start(mem, can_send)

        @pl.when(jnp.logical_not(can_recv))
        def _():
            got_s[r, d] = jnp.zeros(got_s.shape[2:], bf16)
            got_info_s[r, d] = jnp.full(got_info_s.shape[2:], -1.0, f32)

    def state_recv(r, d, far, src, info):
        mem, note, _, can_recv = state_copies(r, d, far, src, info)

        @pl.when(can_recv)
        def _():
            note.wait_recv()
            mem.wait_recv()

    for far in (1, 2):
        for d in (0, 1):
            state_send(far - 1, d, far, own_s, own_info_s)
    send_up(planes[2], 1)
    send_up(planes[1], 1)
    start(over_up(me.z, 1, True))

    q_in.wait()

    def inside(j, carry):
        r0 = pl.multiple_of(j * rows, rows)
        score = (
            lax.dot_general(
                q_s[pl.ds(r0, rows), :],
                k_s[...],
                (((1,), (1,)), ((), ())),
                preferred_element_type=f32,
            )
            * scale
        )
        at_row = lax.broadcasted_iota(jnp.int32, (rows, length), 0) + r0
        at_col = lax.broadcasted_iota(jnp.int32, (rows, length), 1)
        cols = cols_s[pl.ds(r0, rows), :]
        same = cols[:, 2:3] == rows_s[2:3, :]
        for d in (0, 1):
            order = (at_row >= at_col) if d == 0 else (at_row <= at_col)
            exponent = jnp.where(
                same & order, cols[:, d : d + 1] + rows_s[d : d + 1, :], far_low
            )
            top = jnp.max(exponent, axis=1, keepdims=True)
            weights = score * jnp.exp(exponent - top)
            stat_s[2 * d, pl.ds(r0, rows), :] = top
            stat_s[2 * d + 1, pl.ds(r0, rows), :] = jnp.sum(weights, axis=1, keepdims=True)
            num_s[d, pl.ds(r0, rows), :] = jnp.dot(
                weights.astype(bf16), v_s[...], preferred_element_type=f32
            )
        return carry

    lax.fori_loop(0, length // rows, inside, 0)

    def info_row(r, d, i):
        return got_info_s[r, d, i : i + 1, :]

    near = []
    for d in (0, 1):
        here = (first if d == 0 else last)[0:1]
        state_recv(0, d, 1, own_s, own_info_s)
        state_recv(1, d, 2, own_s, own_info_s)
        link1 = info_row(0, d, 3) == here
        link2 = info_row(1, d, 3) == here
        level1 = jnp.where(link1, info_row(0, d, 1), far_low)
        level2 = jnp.where(link2, info_row(1, d, 1) + info_row(0, d, 2), far_low)
        top = jnp.maximum(level1, level2)
        share1 = jnp.where(link1, jnp.exp(level1 - top), 0.0)
        share2 = jnp.where(link2, jnp.exp(level2 - top), 0.0)
        norm = share1 * info_row(0, d, 0) + share2 * info_row(1, d, 0)
        mid_s[d] = (
            share1[:, 0:1] * got_s[0, d].astype(f32) + share2[:, 0:1] * got_s[1, d].astype(f32)
        ).astype(bf16)
        at = lax.broadcasted_iota(jnp.int32, (8, depth), 0)
        mid_info_s[d] = jnp.where(at == 0, norm, jnp.where(at == 1, top, here))
        state_send(2, d, 2, mid_s, mid_info_s)
        near.append((here, top, norm))

    relay_up(planes[2], 0)
    relay_up(planes[1], 0)

    ends = []
    for d in (0, 1):
        here, top, norm = near[d]
        state_recv(2, d, 2, mid_s, mid_info_s)
        link = info_row(2, d, 3) == here
        level = jnp.where(
            link, info_row(2, d, 1) + info_row(1, d, 2) + info_row(0, d, 2), far_low
        )
        peak = jnp.maximum(top, level)
        link1 = info_row(0, d, 3) == here
        share = jnp.where(link1, jnp.exp(top - peak), 0.0)
        share_far = jnp.where(link, jnp.exp(level - peak), 0.0)
        fin_s[d] = (
            share[:, 0:1] * mid_s[d].astype(f32) + share_far[:, 0:1] * got_s[2, d].astype(f32)
        ).astype(bf16)
        meets = jnp.where(link1, here, -2.0)
        ends.append((meets[:, 0:1], peak, share * norm + share_far * info_row(2, d, 0)))

    for h in range(2):
        for i in range(3, line):
            send_up(planes[i], h)
    send_dn(planes[2], 0)
    og_in.wait()

    def project(j):
        r0 = pl.multiple_of(j * rows, rows)
        queries = q_s[pl.ds(r0, rows), :]
        wide_q = queries.astype(f32)
        cols = cols_s[pl.ds(r0, rows), :]
        memory = None
        for d in (0, 1):
            meets, level, norm = ends[d]
            usable = cols[:, 2:3] == meets
            carried = jnp.where(usable, cols[:, d : d + 1] + level[:, 0:1], far_low)
            top = stat_s[2 * d, pl.ds(r0, rows), :]
            peak = jnp.maximum(carried, top)
            local = jnp.exp(top - peak)
            inter = jnp.where(usable, jnp.exp(carried - peak), 0.0) * scale
            den = local * stat_s[2 * d + 1, pl.ds(r0, rows), :] + inter * jnp.sum(
                wide_q * norm, axis=1, keepdims=True
            )
            under = 1.0 / jnp.maximum(jnp.abs(den), 1.0)
            term = (local * under) * num_s[d, pl.ds(r0, rows), :] + (inter * under) * jnp.dot(
                queries, fin_s[d], preferred_element_type=f32
            )
            memory = term if memory is None else memory + term
        normed = memory * lax.rsqrt(jnp.mean(memory * memory, axis=1, keepdims=True) + eps)
        open_gate = jax.nn.sigmoid(og_s[pl.ds(r0, rows), :].astype(f32))
        read_s[j] = (normed * hg_ref[...].reshape(1, width) * open_gate).astype(bf16)

    ro_no = [wire.slot() for _ in range(3)]
    peers = [(far_x, far_c), (far_x, me.c), (me.x, far_c)]

    def exchange(i):
        x, c = peers[i]
        return wire.copy(read_s.at[x * 2 + c], heads_s.at[me.tp], ro_no[i], me.at(x=x, c=c))

    for i in range(3):
        project(peers[i][0] * 2 + peers[i][1])
        start(exchange(i))
    project(me.tp)
    relay_up(planes[1], 1)
    relay_up(planes[2], 1)
    who_wo = far_x * 2 + me.c
    heads_row(wo_no[0], over, who_wo).wait_recv()
    start(heads_row(wo_no[2], core, who_wo))
    res_in.wait()
    wo_in.wait()

    def head_part(rows_ref, owner_tp):
        part = jnp.dot(rows_ref[...], wo_s[owner_tp], preferred_element_type=f32)
        return part.astype(bf16).astype(f32)

    mixed_s[...] = res_s[...].astype(f32) + head_part(read_s.at[me.tp], me.tp)
    for i in (2, 1, 0):
        x, c = peers[i]
        frm = x * 2 + c
        if i == 2:
            heads_row(wo_no[1], core, frm).wait_recv()
        if i == 0:
            heads_row(wo_no[2], core, frm).wait_recv()
        wire.copy(read_s.at[me.tp], heads_s.at[frm], ro_no[i], me.at(x=x, c=c)).wait_recv()
        mixed_s[...] += head_part(heads_s.at[frm], frm)
    mixed = mixed_s[...]
    factor = lax.rsqrt(jnp.mean(mixed * mixed, axis=1, keepdims=True) + eps)
    mine = me.zp * n_tp + me.tp
    nrm_s[mine] = (mixed * factor * ng_ref[...].reshape(1, nrm_s.shape[2])).astype(bf16)

    inner = jnp.where(me.base == 0, 1, me.base)
    others = [
        jnp.where(me.base == 0, 2 + i, lax.rem(me.base + line - 1 - i, line))
        for i in range(line - 2)
    ]
    course = [inner, 2 * me.base + 1 - inner] + others
    order = []
    for z in course:
        order += [(z, me.y), (z, 1 - me.y)]

    def relay_dn(z, h, cond=None):
        ref = dn_s.at[z * 2 + me.y, dn_part[h]]
        got = wire.copy(ref, ref, dn_z[h] + z, me.at(z=z))
        if cond is None:
            got.wait_recv()
        else:
            pl.when(cond)(got.wait_recv)
        start(over_dn(z, h), cond)

    blocks = n_sp
    r1_no = [wire.slot() for _ in range(blocks)]
    r2_no = [wire.slot() for _ in range(blocks)]
    r3_no = [wire.slot() for _ in range(blocks)]
    split = 4
    r1_far = [wire.slot() for _ in range(split)][0]
    r2_far = [wire.slot() for _ in range(split)][0]
    r1_near, r2_near = r1_no[0], r2_no[0]
    first_own = jnp.where(me.z == inner, 0, 2)
    far_z = 1 - me.zp

    def r1_part(k, zp, number):
        pair = pl.ds(zp * 2, 2)
        return wire.copy(part_s.at[k, far_c, pair], r1_s.at[k, pair], number + k, core)

    def r2_part(k, zp, number):
        return wire.copy(r2_out_s.at[k, zp], r2_in_s.at[k, zp], number + k, over)

    def part_dot(k, slot, zp, number):
        for x in range(2):
            g = zp * 2 + x
            value = jnp.dot(hid_s[g], dn_s[slot], preferred_element_type=f32).astype(bf16)
            part_s[k, 0, g] = value[:rows]
            part_s[k, 1, g] = value[rows:]
        r1_part(k, zp, number).start()

    def part_sum(k, zp, first, second):
        r1_part(k, zp, first).wait_recv()

        def both(g):
            return part_s[k, me.c, g].astype(f32) + r1_s[k, g].astype(f32)

        r2_out_s[k, zp] = both(zp * 2 + far_x).astype(bf16)
        r2_part(k, zp, second).start()
        r2_keep_s[k, zp] = both(zp * 2 + me.x)

    for k in range(split):
        waits.append((r1_part(k, me.zp, r1_near), None))
        waits.append((r1_part(k, far_z, r1_far), None))
        waits.append((r2_part(k, me.zp, r2_near), None))
        waits.append((r2_part(k, far_z, r2_far), None))

    def owner(zp, x, c):
        return zp * n_tp + x * 2 + c

    n_core = [wire.slot() for _ in range(2)]
    n_x = wire.slot()
    n_z, n_xz = [wire.slot(), wire.slot()], [wire.slot(), wire.slot()]
    n_corez, n_corexz = [wire.slot(), wire.slot()], [wire.slot(), wire.slot()]
    half = rows // 2
    parts = [pl.ds(0, half), pl.ds(half, half)]

    def pass_on(number, where, who, part=None):
        ref = nrm_s.at[who] if part is None else nrm_s.at[who, part]
        return wire.copy(ref, ref, number, where)

    start(pass_on(n_x, over, mine))
    for h in range(2):
        start(pass_on(n_z[h], above, mine, parts[h]))
    start(pass_on(n_core[0], core, mine))
    for h in range(2):
        send_dn(planes[1], h)
    for h in range(2):
        start(over_dn(me.z, h, True))
    for h in range(2):
        for i in range(3, line):
            relay_up(planes[i], h)

    def raise_rows(zp, x):
        group = zp * 2 + x

        def chunk(n, carry):
            c0 = pl.multiple_of(n * 256, 256)
            left = nrm_s[pl.ds(group * 2, 2), :, :].reshape(2 * rows, nrm_s.shape[2])
            right = up_s[:, :, pl.ds(c0, 256)].reshape(n_sp * deep, 256)
            pre = jnp.maximum(jnp.dot(left, right, preferred_element_type=f32), 0.0)
            hid_s[group, :, pl.ds(c0, 256)] = (pre * pre).astype(bf16)
            return carry

        lax.fori_loop(0, hidden // 256, chunk, 0)

    who = owner(me.zp, far_x, me.c)
    pass_on(n_x, over, who).wait_recv()
    start(pass_on(n_core[1], core, who))
    for h in range(2):
        for i in range(3, line):
            send_dn(planes[i], h, inner_line)
    relay_dn(planes[2], 0)
    who = owner(far_z, me.x, me.c)
    for h in range(2):
        pass_on(n_z[h], above, who, parts[h]).wait_recv()
        start(pass_on(n_xz[h], over, who, parts[h]))
        start(pass_on(n_corez[h], core, who, parts[h]))
    for copy in own_in:
        copy.wait()
    for z in planes:
        for h in range(2):
            crossed_up(z, h)
    pass_on(n_core[0], core, owner(me.zp, me.x, far_c)).wait_recv()
    raise_rows(me.zp, me.x)
    send_dn(planes[2], 1)
    pass_on(n_core[1], core, owner(me.zp, far_x, far_c)).wait_recv()
    raise_rows(me.zp, far_x)
    for h in range(2):
        pass_on(n_corez[h], core, owner(far_z, me.x, far_c), parts[h]).wait_recv()
    raise_rows(far_z, me.x)
    for h in range(2):
        relay_dn(planes[1], h)
    for copy in dn_in:
        copy.wait()
    for h in range(2):
        crossed_dn(me.z, h)
    part_dot(first_own, me.sp, me.zp, r1_near)
    part_dot(first_own + 1, me.z * 2 + 1 - me.y, me.zp, r1_near)
    who = owner(far_z, far_x, me.c)
    for h in range(2):
        pass_on(n_xz[h], over, who, parts[h]).wait_recv()
        start(pass_on(n_corexz[h], core, who, parts[h]))
    for h in range(2):
        pass_on(n_corexz[h], core, owner(far_z, far_x, far_c), parts[h]).wait_recv()
    part_sum(first_own, me.zp, r1_near, r2_near)
    part_sum(first_own + 1, me.zp, r1_near, r2_near)
    raise_rows(far_z, far_x)

    groups = 4

    def lower(k):
        z, y = order[k]
        if k == 0:
            for h in range(2):
                for i in range(3, line):
                    send_dn(planes[i], h, ends_line)
        if k == 1:
            for h in range(2):
                for i in range(3, line):
                    relay_dn(planes[i], h, inner_line)
        if k == 3:
            relay_dn(planes[2], 1)
        if k in (4, 5):
            for i in range(3, line):
                relay_dn(planes[i], k - 4, ends_line)
        slot = z * 2 + y
        if k < split:

            @pl.when(z != me.z)
            def _():
                if k % 2 == 1:
                    for h in range(2):
                        crossed_dn(z, h)
                part_dot(k, slot, me.zp, r1_near)

            part_dot(k, slot, far_z, r1_far)
            return
        if k % 2 == 1:
            for h in range(2):
                crossed_dn(z, h)

        def one(g, carry):
            value = jnp.dot(hid_s[g], dn_s[slot], preferred_element_type=f32).astype(bf16)
            part_s[k, 0, g] = value[:rows]
            part_s[k, 1, g] = value[rows:]
            return carry

        lax.fori_loop(0, groups, one, 0)
        start(wire.copy(part_s.at[k, far_c], r1_s.at[k], r1_no[k], core))

    def over_x(k):
        return k < split or k % 2 == 1

    def sum1(k):
        if k < split:

            @pl.when(order[k][0] != me.z)
            def _():
                part_sum(k, me.zp, r1_near, r2_near)

            part_sum(k, far_z, r1_far, r2_far)
            return
        wire.copy(part_s.at[k, far_c], r1_s.at[k], r1_no[k], core).wait_recv()

        def both(g):
            return part_s[k, me.c, g].astype(f32) + r1_s[k, g].astype(f32)

        for i in range(2):
            away = i * 2 + far_x if over_x(k) else far_z * 2 + i
            r2_out_s[k, i] = both(away).astype(bf16)
        start(wire.copy(r2_out_s.at[k], r2_in_s.at[k], r2_no[k], over if over_x(k) else above))
        for i in range(2):
            here = i * 2 + me.x if over_x(k) else me.zp * 2 + i
            r2_keep_s[k, i] = both(here)

    def sum2(k):
        first, second = (over, above) if over_x(k) else (above, over)
        if k < split:
            r2_part(k, me.zp, r2_near).wait_recv()
            r2_part(k, far_z, r2_far).wait_recv()
        else:
            wire.copy(r2_out_s.at[k], r2_in_s.at[k], r2_no[k], first).wait_recv()
        far = far_z if over_x(k) else far_x
        r3_out_s[k] = (r2_keep_s[k, far] + r2_in_s[k, far].astype(f32)).astype(bf16)
        start(wire.copy(r3_out_s.at[k], r3_in_s.at[k], r3_no[k], second))

    def sum3(k):
        second = above if over_x(k) else over
        wire.copy(r3_out_s.at[k], r3_in_s.at[k], r3_no[k], second).wait_recv()
        z, y = order[k]
        c0 = pl.multiple_of((z * 2 + y) * wide, wide)
        at = me.zp if over_x(k) else me.x
        total = r2_keep_s[k, at] + r2_in_s[k, at].astype(f32) + r3_in_s[k].astype(f32)
        total = mixed_s[:, pl.ds(c0, wide)] + total
        out_ref[:, pl.ds(c0, wide)] = total.astype(bf16)

    for k in range(blocks + 4):
        if 0 <= k - 1 < blocks:
            sum1(k - 1)
        if k < blocks:
            lower(k)
        if 0 <= k - 2 < blocks:
            sum2(k - 2)
        if 0 <= k - 4 < blocks:
            sum3(k - 4)

    for copy, cond in waits:
        if cond is None:
            copy.wait_send()
        else:
            pl.when(cond)(copy.wait_send)


def fused(n_sp, n_tp, *args):
    (
        queries,
        keys,
        values,
        out_gate,
        input_gates,
        forget_gates,
        doc_ids,
        head_gain,
        w_out,
        resid,
        norm_gain,
        w_up,
        w_down,
    ) = args
    length, depth = queries.shape
    width = values.shape[1]
    rows, model = resid.shape
    deep, wide = w_up.shape[0], w_down.shape[1]
    hidden = w_up.shape[1] // 2
    line = n_sp // 2
    blocks = n_sp
    numbers = 8 * line + 40 + 3 * blocks
    vmem = pltpu.VMEM
    scratch = [
        vmem((length, depth), bf16),
        vmem((length, depth), bf16),
        vmem((length, width), bf16),
        vmem((length, width), bf16),
        vmem((n_tp, width, model), bf16),
        vmem((rows, model), bf16),
        vmem((n_sp, deep, hidden), bf16),
        vmem((n_sp, hidden, wide), bf16),
        vmem((8, length), f32),
        vmem((length, 8), f32),
        vmem((2, length, width), f32),
        vmem((4, length, 1), f32),
        vmem((2, depth, width), bf16),
        vmem((2, 8, depth), f32),
        vmem((3, 2, depth, width), bf16),
        vmem((3, 2, 8, depth), f32),
        vmem((2, depth, width), bf16),
        vmem((2, 8, depth), f32),
        vmem((2, depth, width), bf16),
        vmem((n_tp, rows, width), bf16),
        vmem((n_tp, rows, width), bf16),
        vmem((rows, model), f32),
        vmem((2 * n_tp, rows, model), bf16),
        vmem((4, 2 * rows, hidden), bf16),
        vmem((blocks, 2, 4, rows, wide), bf16),
        vmem((blocks, 4, rows, wide), bf16),
        vmem((blocks, 2, rows, wide), bf16),
        vmem((blocks, 2, rows, wide), f32),
        vmem((blocks, 2, rows, wide), bf16),
        vmem((blocks, rows, wide), bf16),
        vmem((blocks, rows, wide), bf16),
        pltpu.SemaphoreType.DMA((10,)),
        pltpu.SemaphoreType.DMA((numbers,)),
        pltpu.SemaphoreType.DMA((numbers,)),
    ]
    anywhere = pl.BlockSpec(memory_space=pl.ANY)
    inside = pl.BlockSpec(memory_space=pltpu.VMEM)
    return pl.pallas_call(
        functools.partial(layer_kernel, n_sp, n_tp),
        out_shape=jax.ShapeDtypeStruct((rows, model), bf16),
        in_specs=[anywhere] * 4 + [inside] * 4 + [anywhere] * 2 + [inside] + [anywhere] * 2,
        out_specs=inside,
        scratch_shapes=scratch,
        compiler_params=pltpu.CompilerParams(
            collective_id=0, has_side_effects=True, vmem_limit_bytes=66_000_000
        ),
        name="layer",
    )(
        queries,
        keys,
        values,
        out_gate,
        input_gates,
        forget_gates,
        doc_ids,
        head_gain,
        w_out,
        resid,
        norm_gain,
        w_up,
        w_down,
    )


def fits(mesh, args):
    n_sp, n_tp = mesh.shape["sp"], mesh.shape["tp"]
    queries, input_gates, w_up, w_down = args[0], args[4], args[11], args[12]
    length = queries.shape[0] // n_sp
    return (
        n_tp == 4
        and n_sp % 4 == 0
        and input_gates.shape[1] == n_tp
        and -(-longest_doc // length) <= 4
        and length % (n_tp * 32) == 0
        and w_down.shape[1] % (n_sp * 128) == 0
        and w_up.shape[0] % (n_sp * 16) == 0
        and w_up.shape[1] % (n_tp * 512) == 0
    )


def solution(mesh):
    in_specs = (
        P("sp", "tp"),
        P("sp", "tp"),
        P("sp", "tp"),
        P("sp", "tp"),
        P(None, "tp", "sp"),
        P(None, "tp", "sp"),
        P("sp"),
        P("tp"),
        P("tp", None),
        P(("sp", "tp"), None),
        P(),
        P("sp", "tp"),
        P("tp", "sp"),
    )
    out_specs = P(("sp", "tp"), None)

    def step(*args):
        whole = fits(mesh, args)
        body = functools.partial(fused, mesh.shape["sp"], mesh.shape["tp"]) if whole else shards
        return jax.shard_map(
            body, mesh=mesh, in_specs=in_specs, out_specs=out_specs, check_vma=False
        )(*args)

    return step
```
